512 devices in a mesh: sp: 16 (over z), dp: 32 (over y, x, core).
Axes of the slice: x: 4, y: 4, z: 16, core: 2. Of those that a mesh axis runs over, the one named last changes fastest.
Arguments:
- normed: bfloat16 [32, 1024, 2048], P('dp', None, 'sp'), may hold values from -6 to 6
- branch_in: bfloat16 [32, 1024, 2048], P('dp', 'sp'), may hold values from -12 to 12
- gate_pre: bfloat16 [32, 1024, 2048], P('dp', 'sp'), may hold values from -6 to 6
- cotangent: bfloat16 [32, 1024, 2048], P('dp', None, 'sp'), may hold values from -6 to 6
- decay_shift: float32 [32, 16, 2048], P('dp', 'sp'), may hold values from -1.2 to -9.765625e-05
- conv_weight: float32 [4, 1024], P(None, 'sp'), may hold values from -3 to 3
- recur_weight: float32 [16, 64, 64], P('sp'), may hold values from -0.75 to 0.75
- input_weight: float32 [16, 64, 64], P('sp'), may hold values from -0.75 to 0.75
- decay_param: float32 [1024], P('sp')
- branch_proj: bfloat16 [1024, 1024], P('dp'), may hold values from -0.1875 to 0.1875
Outputs:
- grad_normed: bfloat16 [32, 1024, 2048], P('dp', None, 'sp')
- grad_gate: bfloat16 [32, 1024, 2048], P('dp', 'sp')
- grad_proj: float32 [1024, 1024], P('dp', 'sp')
- grad_conv: float32 [4, 1024], P(None, 'sp')
- grad_recur: float32 [16, 64, 64], P('sp')
- grad_input: float32 [16, 64, 64], P('sp')
- grad_decay: float32 [1024], P('sp')
The draws below stay inside these ranges and needn't reach their ends.
All inputs are finite; a program needn't handle non-finite values.
Results may differ from the reference program's by a relative error of at most 0.019.
Values may be sent and summed in bfloat16 or wider, within the bound.
No kernel may reach another device: no remote copies, remote signals or barrier semaphores. Data moves between devices by JAX's collectives and lax.ppermute only.
A program may use at most 64 MiB of HBM per device.

```python
import jax
import jax.numpy as jnp
from jax import lax

D = 1024
REC_BLOCKS = 16
BLOCK_W = 64
CONV = 4
TOK_DEV = 128
D_REC = 1024
LENGTH = 2048
SEQS = 32


def draw_branch_in(key, part):
    first, second = jax.random.split(jax.random.fold_in(key, 3))
    spans = LENGTH // TOK_DEV
    factor = jnp.exp(jax.random.uniform(second, (SEQS, 1, spans), jnp.float32, -0.6, 0.6))
    factor = jnp.repeat(factor, TOK_DEV, axis=2)
    values = jax.random.normal(first, (SEQS, D_REC, LENGTH), jnp.float32)
    return (values * factor).astype(jnp.bfloat16)


def draw_decay_shift(key, part):
    first, second, third = jax.random.split(jax.random.fold_in(key, 11), 3)
    spans = LENGTH // TOK_DEV
    base = -jax.random.uniform(first, (SEQS, REC_BLOCKS, spans), jnp.float32, 0.2, 1.0) / LENGTH
    base = jnp.repeat(base, TOK_DEV, axis=2)
    where = jax.random.randint(second, (SEQS, REC_BLOCKS, 2), 0, LENGTH)
    depth = jnp.log(jax.random.uniform(third, (SEQS, REC_BLOCKS, 2), jnp.float32, 0.55, 0.8))
    places = jnp.arange(LENGTH)
    hits = (places[None, None, None, :] == where[:, :, :, None]).astype(jnp.float32)
    return base + jnp.sum(hits * depth[:, :, :, None], axis=2)


def draw_decay_param(key, part):
    first, second, third = jax.random.split(jax.random.fold_in(key, 7), 3)
    share = 0.5
    quick = jax.random.bernoulli(first, share, (D_REC,))
    quick_rate = jnp.exp(jax.random.uniform(second, (D_REC,), jnp.float32, jnp.log(2.5), jnp.log(8.0))) / TOK_DEV
    slow_rate = jnp.exp(jax.random.uniform(third, (D_REC,), jnp.float32, jnp.log(0.1), jnp.log(0.6))) / LENGTH
    softened = jnp.where(quick, quick_rate, slow_rate) / 4.0
    return -jnp.log(jnp.expm1(softened))


def spiked(entries, rng, source, target, parts, factor):
    def block_of(position):
        return (jnp.arange(entries.shape[position]) // (entries.shape[position] // parts)).reshape((-1,) + (1,) * (entries.ndim - 1 - position))

    first = jax.random.permutation(rng, parts)[block_of(target)]
    far = (block_of(target) + parts // 2) % parts
    return jnp.where((block_of(source) == first) | (block_of(source) == far), factor * entries, entries)


def steps_of(rng, extent, pieces, smallest, top_value):
    level = 1.0
    for dim, blocks in pieces:
        steps = jax.random.uniform(jax.random.fold_in(jax.random.fold_in(rng, 6), dim), (blocks,), jnp.float32, smallest / len(pieces), top_value / len(pieces))
        level = level * jnp.repeat(jnp.exp(steps), extent[dim] // blocks).reshape((-1,) + (1,) * (len(extent) - 1 - dim))
    return level


def centred(key, extent, width, reach, shards=(), held_as=jnp.bfloat16):
    entries = width * jax.random.normal(key, extent, jnp.float32)
    if shards:
        entries = entries * steps_of(key, extent, shards, -0.22, 0.18)
    return jnp.clip(entries, -reach, reach).astype(held_as)


def gaussian_with(stream_key, extent, spread, limit, pieces, heavy, dtype=jnp.bfloat16):
    values = spread * jax.random.normal(stream_key, extent, jnp.float32)
    if pieces:
        values = values * steps_of(stream_key, extent, pieces, -0.22, 0.18)
    return jnp.clip(spiked(values, jax.random.fold_in(stream_key, 3), *heavy), -limit, limit).astype(dtype)


def setup_inputs(seed: int = 0) -> dict:
    seeds = jax.random.split(jax.random.key(seed), 11)
    normed = gaussian_with(seeds[0], (SEQS, D, LENGTH), 1.0, 6.0, ((0, 32), (2, 16)), (0, 1, 32, 2.75))
    branch_in = draw_branch_in(jax.random.fold_in(seeds[10], 71), 0)
    gate_pre = centred(seeds[2], (SEQS, D_REC, LENGTH), 1.0, 6.0, ((0, 32), (1, 16)))
    cotangent = gaussian_with(seeds[3], (SEQS, D_REC, LENGTH), 1.0, 6.0, ((0, 32), (2, 16)), (2, 1, 16, 2.0))
    decay_shift = draw_decay_shift(jax.random.fold_in(seeds[10], 71), 0)
    conv_weight = centred(seeds[5], (CONV, D_REC), CONV ** -0.5, 3.0, ((1, 16),), jnp.float32)
    recur_weight = centred(seeds[6], (REC_BLOCKS, BLOCK_W, BLOCK_W), BLOCK_W ** -0.5, 0.75, ((0, 16),), jnp.float32)
    input_weight = centred(seeds[7], (REC_BLOCKS, BLOCK_W, BLOCK_W), BLOCK_W ** -0.5, 0.75, ((0, 16),), jnp.float32)
    decay_param = draw_decay_param(jax.random.fold_in(seeds[10], 71), 0)
    branch_proj = centred(seeds[9], (D, D_REC), D ** -0.5, 0.1875, ((0, 32),))
    return dict(normed=normed, branch_in=branch_in, gate_pre=gate_pre, cotangent=cotangent, decay_shift=decay_shift, conv_weight=conv_weight, recur_weight=recur_weight, input_weight=input_weight, decay_param=decay_param, branch_proj=branch_proj)


gate_const = 8.0
highest = lax.Precision.HIGHEST

def mixer(branch, gate, shift, conv_weight, recur_weight, input_weight, decay_param):
    channels, length = branch.shape
    values = branch.astype(jnp.float32)
    padded = jnp.pad(values, ((0, 0), (CONV - 1, 0)))
    convolved = conv_weight[0][:, None] * padded[:, 0:length]
    for offset in range(1, CONV):
        convolved = convolved + conv_weight[offset][:, None] * padded[:, offset:offset + length]
    groups = channels // BLOCK_W
    grouped = convolved.reshape(groups, BLOCK_W, length)
    recur_gate = jax.nn.sigmoid(jnp.einsum('gil,gij->gjl', grouped, recur_weight, precision=highest).reshape(channels, length))
    input_gate = jax.nn.sigmoid(jnp.einsum('gil,gij->gjl', grouped, input_weight, precision=highest).reshape(channels, length))
    log_decay = -gate_const * recur_gate * jax.nn.softplus(-decay_param)[:, None] + jnp.repeat(shift, BLOCK_W, axis=0)
    decay = jnp.exp(log_decay)
    pushed = jnp.sqrt(-jnp.expm1(2.0 * log_decay)) * input_gate * convolved

    def combine(earlier, later):
        return (earlier[0] * later[0], later[0] * earlier[1] + later[1])
    _, states = lax.associative_scan(combine, (decay, pushed), axis=1)
    return states * jax.nn.gelu(gate.astype(jnp.float32))

def mixer_grads(branch, gate, shift, upstream, conv_weight, recur_weight, input_weight, decay_param):

    def local(branch_f, gate_f, conv_f, recur_f, input_f, decay_f):
        return mixer(branch_f, gate_f, shift, conv_f, recur_f, input_f, decay_f)
    _, pullback = jax.vjp(local, branch.astype(jnp.float32), gate.astype(jnp.float32), conv_weight, recur_weight, input_weight, decay_param)
    return pullback(upstream.astype(jnp.float32))

def reference(normed, branch_in, gate_pre, cotangent, decay_shift, conv_weight, recur_weight, input_weight, decay_param, branch_proj):

    def per_sequence(carry, items):
        seq_normed, seq_branch, seq_gate, seq_cot, seq_shift = items
        grad_branch, grad_gate, grad_conv, grad_recur, grad_input, grad_decay = mixer_grads(seq_branch, seq_gate, seq_shift, seq_cot, conv_weight, recur_weight, input_weight, decay_param)
        branch_rounded = grad_branch.astype(jnp.bfloat16)
        grad_normed = jnp.dot(branch_proj, branch_rounded, preferred_element_type=jnp.float32).astype(jnp.bfloat16)
        proj_term = lax.dot_general(seq_normed, branch_rounded, (((1,), (1,)), ((), ())), preferred_element_type=jnp.float32)
        carry = (carry[0] + proj_term, carry[1] + grad_conv, carry[2] + grad_recur, carry[3] + grad_input, carry[4] + grad_decay)
        return (carry, (grad_normed, grad_gate.astype(jnp.bfloat16)))
    start = (jnp.zeros((D, D_REC), jnp.float32), jnp.zeros((CONV, D_REC), jnp.float32), jnp.zeros((REC_BLOCKS, BLOCK_W, BLOCK_W), jnp.float32), jnp.zeros((REC_BLOCKS, BLOCK_W, BLOCK_W), jnp.float32), jnp.zeros((D_REC,), jnp.float32))
    totals, outputs = lax.scan(per_sequence, start, (normed, branch_in, gate_pre, cotangent, decay_shift))
    return (outputs[0], outputs[1], totals[0], totals[1], totals[2], totals[3], totals[4])
```

```python
import jax
import jax.numpy as jnp
from jax import lax
from jax.experimental import pallas as pl
from jax.experimental.pallas import tpu as pltpu
from jax.sharding import Mesh
from jax.sharding import PartitionSpec as P

SPAN = 128
GROUP = 64
CONV = 4
GATE = 8.0
f32 = jnp.float32
bf16 = jnp.bfloat16
DP = ("y", "x", "core")
NEAREST = (0, 1, 3, 2)


def lanes(shape):
    return lax.broadcasted_iota(jnp.int32, shape, 1)


def high_low(value):
    high = value.astype(bf16)
    return high, (value - high.astype(f32)).astype(bf16)


def strided(ref, n):
    return ref[pl.ds(n, SPAN, stride=8), :]


def before_of(block):
    row = lax.broadcasted_iota(jnp.int32, block.shape, 0)
    lane = lanes(block.shape)
    moved = pltpu.roll(block, 1, 0)
    across = jnp.where(lane >= GROUP, pltpu.roll(moved, GROUP, 1), 0.0)
    return jnp.where(row == 0, across, moved)


def after_of(block):
    row = lax.broadcasted_iota(jnp.int32, block.shape, 0)
    lane = lanes(block.shape)
    moved = pltpu.roll(block, 7, 0)
    across = jnp.where(lane < GROUP, pltpu.roll(moved, GROUP, 1), 0.0)
    return jnp.where(row == 7, across, moved)


def entering(factor, value, backward):
    row = lax.broadcasted_iota(jnp.int32, factor.shape, 0)
    lane = lanes(factor.shape)
    a, b = factor, value
    for step in (1, 2, 4):
        inside = row < 8 - step if backward else row >= step
        shift = 8 - step if backward else step
        b = b + a * jnp.where(inside, pltpu.roll(b, shift, 0), 0.0)
        a = a * jnp.where(inside, pltpu.roll(a, shift, 0), 1.0)
    edge = b[0:1] if backward else b[7:8]
    later = lane < GROUP if backward else lane >= GROUP
    base = jnp.where(later, jnp.broadcast_to(pltpu.roll(edge, GROUP, 1), factor.shape), 0.0)
    total = b + a * base
    return after_of(total) if backward else before_of(total)


def block_of(n):
    return pl.ds(pl.multiple_of(n * SPAN, SPAN), SPAN)


def moved_block(n, rows):
    return pl.ds(pl.multiple_of(n * SPAN + rows, 8), SPAN)


def tiled(row):
    return jnp.broadcast_to(row, (SPAN, SPAN))


def halves(top, low):
    return jnp.concatenate([top, low], axis=0)


def forward_kernel(
    branch, gate, shift, conv, decay_param, recur_map, input_map,
    next_o, c0_o, c1_o, c2_o, c3_o, branch_o, turned_o, g0_o, g1_o, back_o, rows,
    b_s, decay_s, fed_s, slope_s, rate_s, recur_s, local_s, power_s,
):
    lane = lanes((GROUP, SPAN))
    minus = -decay_param[...]
    softened = jnp.maximum(minus, 0.0) + jnp.log1p(jnp.exp(-jnp.abs(minus)))
    table = jnp.concatenate(
        [conv[...], -GATE * softened, GATE * (0.5 + 0.5 * jnp.tanh(0.5 * minus)), jnp.zeros((2, GROUP), f32)], axis=0
    )
    rows[...] = jnp.concatenate([table, table], axis=1)
    both = jnp.concatenate([recur_map[...], input_map[...]], axis=1)
    swapped = pltpu.roll(both, GROUP, 1)
    left = lane < GROUP
    first = halves(jnp.where(left, both, 0.0), jnp.where(left, 0.0, swapped))
    second = halves(jnp.where(left, swapped, 0.0), jnp.where(left, 0.0, both))
    w_high, w_low = high_low(jnp.concatenate([first, second], axis=1))
    back_high, back_low = high_low(halves(jnp.transpose(first), jnp.transpose(second)))
    back_o[0] = back_high
    back_o[1] = back_low
    for p in range(8):
        at = slice(p * SPAN, (p + 1) * SPAN)
        far = slice((8 + p) * SPAN, (9 + p) * SPAN)
        b_s[pl.ds(24 + p, SPAN, stride=8), :] = jnp.transpose(
            halves(branch[:, at].astype(f32), branch[:, far].astype(f32))
        )
        fed_s[pl.ds(p, SPAN, stride=8), :] = jnp.transpose(
            halves(
                jnp.broadcast_to(shift[:, at], (GROUP, SPAN)), jnp.broadcast_to(shift[:, far], (GROUP, SPAN))
            )
        )
    for m in range(3):
        b_s[8 * m : 8 * m + 8, :] = before_of(b_s[1024 + 8 * m : 1032 + 8 * m, :])

    def gates(n, _):
        here = block_of(n)
        x = tiled(rows[0:1, :]) * b_s[here, :]
        for k in (1, 2, 3):
            x = x + tiled(rows[k : k + 1, :]) * b_s[moved_block(n, 8 * k), :]
        branch_o[here, :] = b_s[moved_block(n, 24), :].astype(bf16)
        x_high, x_low = high_low(x)
        pre = (
            jnp.dot(x_high, w_high, preferred_element_type=f32)
            + jnp.dot(x_low, w_high, preferred_element_type=f32)
            + jnp.dot(x_high, w_low, preferred_element_type=f32)
        )
        tr = jnp.tanh(0.5 * pre[:, :SPAN])
        ti = jnp.tanh(0.5 * pre[:, SPAN:])
        recur = 0.5 + 0.5 * tr
        inp = 0.5 + 0.5 * ti
        rate = tiled(rows[4:5, :])
        log = rate * recur + fed_s[here, :]
        decay = jnp.exp(log)
        square = decay * decay
        u = 2.0 * log
        series = -u * (1 + u * (1 / 2) * (1 + u * (1 / 3) * (1 + u * (1 / 4) * (1 + u * (1 / 5) * (1 + u * (1 / 6))))))
        left_over = jnp.where(u > -0.25, series, 1.0 - square)
        inverse = lax.rsqrt(left_over)
        root = left_over * inverse
        fed = inp * x
        pushed = root * fed
        decay_s[here, :] = decay
        fed_s[here, :] = pushed
        slope_s[here, :] = square * inverse * fed
        rate_s[here, :] = rate * (0.25 - 0.25 * tr * tr)
        recur_s[here, :] = recur
        c0_o[here, :] = (root * inp).astype(bf16)
        c1_o[here, :] = (pushed * (0.5 - 0.5 * ti)).astype(bf16)
        turned_o[:, here] = jnp.transpose(x).astype(bf16)
        return 0

    lax.fori_loop(0, 8, gates, 0)

    local_s[0:8, :] = jnp.zeros((8, SPAN), f32)
    power_s[0:8, :] = jnp.ones((8, SPAN), f32)

    def scan(n, held):
        value, power = held
        for m in range(8):
            at = pl.ds(pl.multiple_of(n * 64 + 8 * m, 8), 8)
            a = decay_s[at, :]
            value = fed_s[at, :] + a * value
            power = a * power
            to = pl.ds(pl.multiple_of(n * 64 + 8 * m + 8, 8), 8)
            local_s[to, :] = value
            power_s[to, :] = power
        return value, power

    value, power = lax.fori_loop(0, 16, scan, (jnp.zeros((8, SPAN), f32), jnp.ones((8, SPAN), f32)))
    enters = jnp.broadcast_to(entering(power, value, False)[None], (16, 8, SPAN)).reshape(SPAN, SPAN)

    def slopes(n, _):
        here = block_of(n)
        previous = local_s[here, :] + power_s[here, :] * enters
        decay = decay_s[here, :]
        slope = previous * decay - slope_s[here, :]
        c2_o[here, :] = (slope * rate_s[here, :]).astype(bf16)
        c3_o[here, :] = (slope * recur_s[here, :]).astype(bf16)
        fed_s[here, :] = local_s[moved_block(n, 8), :] + power_s[moved_block(n, 8), :] * enters
        return 0

    lax.fori_loop(0, 8, slopes, 0)
    next_o[0:1016, :] = decay_s[8:1024, :]
    next_o[1016:1024, :] = after_of(decay_s[0:8, :])
    for p in range(8):
        state = jnp.transpose(strided(fed_s, p))
        for half, at in ((0, slice(p * SPAN, (p + 1) * SPAN)), (1, slice((8 + p) * SPAN, (9 + p) * SPAN))):
            g = gate[:, at].astype(f32)
            c = 0.7978845608028654
            inner = jnp.tanh(c * (g + 0.044715 * (g * g * g)))
            part = 0.5 + 0.5 * inner
            turn = part + 0.5 * g * (1.0 - inner * inner) * (c * (1.0 + 3 * 0.044715 * (g * g)))
            g0_o[:, at] = (g * part).astype(bf16)
            g1_o[:, at] = (state[GROUP * half : GROUP * half + GROUP] * turn).astype(bf16)


def backward_kernel(
    cot, next_r, c0_r, c1_r, c2_r, c3_r, branch_r, turned_r, g0_r, g1_r, back_r, rows,
    gb_o, gate_o, small_o, d_s, local_s, power_s, dx_s, pushed_s,
):
    for p in range(8):
        parts = []
        for j in (p, 8 + p):
            at = slice(j * SPAN, (j + 1) * SPAN)
            c = cot[j].astype(f32)
            gate_o[:, at] = (c * g1_r[:, at].astype(f32)).astype(bf16)
            parts.append(c * g0_r[:, at].astype(f32))
        d_s[pl.ds(p, SPAN, stride=8), :] = jnp.transpose(halves(*parts))

    def scan(n, held):
        value, power = held
        for m in range(8):
            at = pl.ds(pl.multiple_of(1016 - n * 64 - 8 * m, 8), 8)
            a = next_r[at, :]
            value = d_s[at, :] + a * value
            power = a * power
            local_s[at, :] = value
            power_s[at, :] = power
        return value, power

    value, power = lax.fori_loop(0, 16, scan, (jnp.zeros((8, SPAN), f32), jnp.ones((8, SPAN), f32)))
    enters = jnp.broadcast_to(entering(power, value, True)[None], (16, 8, SPAN)).reshape(SPAN, SPAN)

    def summed(block):
        return jnp.sum(block.reshape(16, 8, SPAN), axis=0)

    def spread(n, total):
        here = block_of(n)
        grad = local_s[here, :] + power_s[here, :] * enters
        high = jnp.concatenate(
            [(grad * c2_r[here, :].astype(f32)).astype(bf16), (grad * c1_r[here, :].astype(f32)).astype(bf16)], axis=1
        )
        pushed_s[here, :] = high
        back = jnp.dot(high, back_r[0], preferred_element_type=f32) + jnp.dot(
            high, back_r[1], preferred_element_type=f32
        )
        dx_s[here, :] = grad * c0_r[here, :].astype(f32) + back
        return total + summed(grad * c3_r[here, :].astype(f32))

    zero = jnp.zeros((8, SPAN), f32)
    decays = lax.fori_loop(0, 8, spread, zero)
    for m in range(3):
        dx_s[1024 + 8 * m : 1032 + 8 * m, :] = after_of(dx_s[8 * m : 8 * m + 8, :])

    def taps(n, totals):
        here = block_of(n)
        value = branch_r[here, :].astype(f32)
        gb, out = None, []
        for k in range(CONV):
            dx = dx_s[moved_block(n, 8 * (3 - k)), :]
            term = tiled(rows[k : k + 1, :]) * dx
            gb = term if gb is None else gb + term
            out.append(totals[k] + summed(value * dx))
        d_s[here, :] = gb
        return tuple(out)

    totals = lax.fori_loop(0, 8, taps, (zero,) * CONV)
    for p in range(8):
        gb = jnp.transpose(strided(d_s, p)).astype(bf16)
        gb_o[p] = gb[:GROUP]
        gb_o[8 + p] = gb[GROUP:]
    product = jnp.dot(turned_r[...], pushed_s[...], preferred_element_type=f32)
    low = lanes((GROUP, SPAN)) < GROUP
    r_part = product[:GROUP, :SPAN] + pltpu.roll(product[GROUP:, :SPAN], GROUP, 1)
    i_part = pltpu.roll(product[:GROUP, SPAN:], GROUP, 1) + product[GROUP:, SPAN:]
    small_o[0:GROUP, :] = jnp.where(low, r_part, i_part).astype(bf16)
    row = lax.broadcasted_iota(jnp.int32, (8, SPAN), 0)
    table = zero
    for k, total in enumerate((*totals, decays * jnp.broadcast_to(rows[5:6, :], (8, SPAN)))):
        flat = jnp.broadcast_to(jnp.sum(total, axis=0, keepdims=True), (8, SPAN))
        table = jnp.where(row == k, flat + pltpu.roll(flat, GROUP, 1), table)
    small_o[GROUP : GROUP + 8, :] = table.astype(bf16)


VMEM = pl.BlockSpec(memory_space=pltpu.VMEM)
FLAT = (1024, SPAN)


def forward_part(branch, gate, shift, conv, decay_param, recur_map, input_map):
    flat = jax.ShapeDtypeStruct(FLAT, bf16)
    plain = jax.ShapeDtypeStruct(branch.shape, bf16)
    return pl.pallas_call(
        forward_kernel,
        out_shape=[
            jax.ShapeDtypeStruct(FLAT, f32),
            *[flat] * 5,
            jax.ShapeDtypeStruct((SPAN, 1024), bf16),
            plain,
            plain,
            jax.ShapeDtypeStruct((2, 2 * SPAN, SPAN), bf16),
            jax.ShapeDtypeStruct((8, SPAN), f32),
        ],
        scratch_shapes=[pltpu.VMEM((1048, SPAN), f32)] + [pltpu.VMEM(FLAT, f32)] * 5 + [pltpu.VMEM((1032, SPAN), f32)] * 2,
        name="forward_part",
    )(branch, gate, shift, conv, decay_param, recur_map, input_map)


def backward_part(cot, saved):
    return pl.pallas_call(
        backward_kernel,
        out_shape=[
            jax.ShapeDtypeStruct((16, GROUP, SPAN), bf16),
            jax.ShapeDtypeStruct((GROUP, 2048), bf16),
            jax.ShapeDtypeStruct((GROUP + 8, 2 * GROUP), bf16),
        ],
        scratch_shapes=[pltpu.VMEM(FLAT, f32)] * 3 + [pltpu.VMEM((1048, SPAN), f32), pltpu.VMEM((1024, 2 * SPAN), bf16)],
        name="backward_part",
    )(cot, *saved)


def product_kernel(place, small, own, near, far, grads, out):
    total = None
    blocks = (own[...], near[...], far[0], far[1])
    for n, block in enumerate(blocks):
        theirs = grads[:, place[0] ^ NEAREST[n]].reshape(256, SPAN)
        term = lax.dot_general(block, theirs, (((1,), (1,)), ((), ())), preferred_element_type=f32)
        total = term if total is None else total + term
    pieces = out.shape[0]
    out[:, 0:32, :] = total.astype(bf16).reshape(pieces, 32, 256)
    top = jnp.concatenate([small[0:32, :], small[32:64, :]], axis=1)
    low = jnp.concatenate([small[64:72, :], jnp.zeros((8, SPAN), bf16)], axis=1)
    out[:, 32:72, :] = jnp.broadcast_to(jnp.concatenate([top, low], axis=0)[None], (pieces, 40, 256))


def gather_sum_kernel(arrived, packed_o, maps_o, rest_o):
    block = lax.broadcasted_iota(jnp.int32, (16, SPAN), 1) // 16
    totals, extra = [], None
    for n in range(4):
        total = arrived[8 * n, 0:32, :].astype(f32)
        for m in range(1, 8):
            total = total + arrived[8 * n + m, 0:32, :].astype(f32)
        totals.append(total)
    for n in range(32):
        term = arrived[n, 32:72, :].astype(f32)
        extra = term if extra is None else extra + term
    maps_o[0:32, :] = extra[0:32, 0:SPAN]
    maps_o[32:64, :] = extra[0:32, SPAN:]
    rest_o[...] = extra[32:40, 0:SPAN]
    for group in range(16):
        tile = slice((group // 8) * SPAN, (group // 8 + 1) * SPAN)
        piece = None
        for j in range(8):
            source = totals[j % 4][16 * (j // 4) : 16 * (j // 4) + 16, tile]
            shift = (16 * (j - group % 8)) % SPAN
            turned = pltpu.roll(source, shift, 1) if shift else source
            piece = turned if piece is None else jnp.where(block == j, turned, piece)
        packed_o[group] = piece.astype(bf16)


def last_sum_kernel(arrived, out):
    total = arrived[0].astype(f32)
    for n in range(1, arrived.shape[0]):
        total = total + arrived[n].astype(f32)
    out[0:16, :] = total[:, 0:GROUP]
    out[16:32, :] = pltpu.roll(total, GROUP, 1)[:, 0:GROUP]


def token_grad_kernel(place, proj, proj_other, own, one, two, three, out, tokens_s):
    for n, piece in enumerate((own, one, two, three)):
        tokens_s[:, (place[0] + 4 - n) % 4] = piece[...]
    tokens = tokens_s[...].reshape(1024, SPAN)
    for k, half in enumerate((proj, proj_other)):
        result = jnp.dot(half[...], tokens, preferred_element_type=f32).astype(bf16)
        for n in range(16):
            y, x = place[0] ^ NEAREST[n % 4], place[1] ^ NEAREST[n // 4]
            row = ((y * 4 + x) * 2 + (place[2] ^ k)) * 32
            out[pl.ds(pl.multiple_of(row, 32), 32), :] = result[32 * n : 32 * n + 32]


def exchanged(array, axis, bit):
    size = lax.axis_size(axis)
    return lax.ppermute(array, axis, [(n, n ^ bit) for n in range(size)])


def joined(array, axis, bits):
    return jnp.concatenate([array, exchanged(array, axis, bits)], axis=0)


def gathered_rows(rows):
    held = joined(joined(rows, "y", 1), "y", 3)
    held = joined(joined(held, "x", 1), "x", 3)
    return held, exchanged(held, "core", 1)


def steps(
    normed, branch_in, gate_pre, cotangent, decay_shift,
    conv_weight, recur_weight, input_weight, decay_param, branch_proj,
):
    spans = lax.axis_size("sp")
    cot = lax.all_to_all(cotangent[0].reshape(spans, GROUP, SPAN), "sp", 0, 0, tiled=True)
    saved = forward_part(
        branch_in[0], gate_pre[0], decay_shift[0], conv_weight, decay_param[None], recur_weight[0], input_weight[0]
    )
    own = normed[0]
    near = exchanged(own, "y", 1)
    far = exchanged(jnp.stack([own, near]), "y", 3)
    gb, grad_gate, small = backward_part(cot, saved)
    grads = lax.all_to_all(gb.reshape(64, 16, SPAN), ("sp", "y"), 0, 0, tiled=True)
    grads = grads.reshape(16, 4, 16, SPAN)
    here = lax.axis_index("y")
    place = jnp.stack([lax.axis_index(axis) for axis in DP]).astype(jnp.int32)
    smem = pl.BlockSpec(memory_space=pltpu.SMEM)
    pieces = pl.pallas_call(
        product_kernel,
        in_specs=[smem] + [VMEM] * 5,
        out_specs=VMEM,
        out_shape=jax.ShapeDtypeStruct((32, 72, 256), bf16),
        name="product",
    )(place, small, own, near, far, grads)
    arrived = lax.all_to_all(pieces, DP, 0, 0, tiled=True)
    own_part = [lax.dynamic_index_in_dim(grads, (here + step) % 4, 1, keepdims=False) for step in range(4)]
    for step in (1, 2, 3):
        own_part[step] = lax.ppermute(own_part[step], "y", [(n, (n + step) % 4) for n in range(4)])
    packed, map_sums, rest = pl.pallas_call(
        gather_sum_kernel,
        out_shape=[
            jax.ShapeDtypeStruct((16, 16, SPAN), bf16),
            jax.ShapeDtypeStruct((GROUP, SPAN), f32),
            jax.ShapeDtypeStruct((8, SPAN), f32),
        ],
        name="gather_sum",
    )(arrived)
    last = lax.all_to_all(packed, "sp", 0, 0, tiled=True)
    grad_proj = pl.pallas_call(
        last_sum_kernel, out_shape=jax.ShapeDtypeStruct((32, GROUP), f32), name="last_sum"
    )(last)
    proj, proj_other = gathered_rows(branch_proj)
    grad_normed = pl.pallas_call(
        token_grad_kernel,
        in_specs=[smem] + [VMEM] * 6,
        out_specs=VMEM,
        out_shape=jax.ShapeDtypeStruct((1024, SPAN), bf16),
        scratch_shapes=[pltpu.VMEM((16, 4, 16, SPAN), bf16)],
        name="token_grad",
    )(place, proj, proj_other, *own_part)
    return (
        grad_normed[None],
        grad_gate[None],
        grad_proj,
        rest[0:CONV, 0:GROUP],
        map_sums[None, :, 0:GROUP],
        map_sums[None, :, GROUP:],
        rest[CONV, 0:GROUP],
    )


def solution(mesh):
    split = Mesh(mesh.devices.reshape(16, 4, 4, 2), ("sp", *DP))
    return jax.shard_map(
        steps,
        mesh=split,
        in_specs=(
            P(DP, None, "sp"),
            P(DP, "sp", None),
            P(DP, "sp", None),
            P(DP, None, "sp"),
            P(DP, "sp", None),
            P(None, "sp"),
            P("sp", None, None),
            P("sp", None, None),
            P("sp"),
            P(DP, None),
        ),
        out_specs=(
            P(DP, None, "sp"),
            P(DP, "sp", None),
            P(DP, "sp"),
            P(None, "sp"),
            P("sp", None, None),
            P("sp", None, None),
            P("sp"),
        ),
        check_vma=False,
    )
```

```python
import jax
import jax.numpy as jnp
from jax import lax
from jax.experimental import pallas as pl
from jax.experimental.pallas import tpu as pltpu
from jax.sharding import Mesh
from jax.sharding import PartitionSpec as P

SPAN = 128
GROUP = 64
CONV = 4
GATE = 8.0
f32 = jnp.float32
bf16 = jnp.bfloat16
DP = ("y", "x", "core")
NEAREST = (0, 1, 3, 2)


def lanes(shape):
    return lax.broadcasted_iota(jnp.int32, shape, 1)


def high_low(value):
    high = value.astype(bf16)
    return high, (value - high.astype(f32)).astype(bf16)


def strided(ref, n):
    return ref[pl.ds(n, SPAN, stride=8), :]


def before_of(block):
    row = lax.broadcasted_iota(jnp.int32, block.shape, 0)
    lane = lanes(block.shape)
    moved = pltpu.roll(block, 1, 0)
    across = jnp.where(lane >= GROUP, pltpu.roll(moved, GROUP, 1), 0.0)
    return jnp.where(row == 0, across, moved)


def after_of(block):
    row = lax.broadcasted_iota(jnp.int32, block.shape, 0)
    lane = lanes(block.shape)
    moved = pltpu.roll(block, 7, 0)
    across = jnp.where(lane < GROUP, pltpu.roll(moved, GROUP, 1), 0.0)
    return jnp.where(row == 7, across, moved)


def entering(factor, value, backward):
    row = lax.broadcasted_iota(jnp.int32, factor.shape, 0)
    lane = lanes(factor.shape)
    a, b = factor, value
    for step in (1, 2, 4):
        inside = row < 8 - step if backward else row >= step
        shift = 8 - step if backward else step
        b = b + a * jnp.where(inside, pltpu.roll(b, shift, 0), 0.0)
        a = a * jnp.where(inside, pltpu.roll(a, shift, 0), 1.0)
    edge = b[0:1] if backward else b[7:8]
    later = lane < GROUP if backward else lane >= GROUP
    base = jnp.where(later, jnp.broadcast_to(pltpu.roll(edge, GROUP, 1), factor.shape), 0.0)
    total = b + a * base
    return after_of(total) if backward else before_of(total)


def block_of(n):
    return pl.ds(pl.multiple_of(n * SPAN, SPAN), SPAN)


def moved_block(n, rows):
    return pl.ds(pl.multiple_of(n * SPAN + rows, 8), SPAN)


def tiled(row):
    return jnp.broadcast_to(row, (SPAN, SPAN))


def halves(top, low):
    return jnp.concatenate([top, low], axis=0)


def forward_kernel(
    branch, gate, shift, conv, decay_param, recur_map, input_map,
    next_o, c0_o, c1_o, c2_o, c3_o, branch_o, turned_o, g0_o, g1_o, back_o, rows,
    b_s, decay_s, fed_s, slope_s, rate_s, recur_s, local_s, power_s,
):
    lane = lanes((GROUP, SPAN))
    minus = -decay_param[...]
    softened = jnp.maximum(minus, 0.0) + jnp.log1p(jnp.exp(-jnp.abs(minus)))
    table = jnp.concatenate(
        [conv[...], -GATE * softened, GATE * (0.5 + 0.5 * jnp.tanh(0.5 * minus)), jnp.zeros((2, GROUP), f32)], axis=0
    )
    rows[...] = jnp.concatenate([table, table], axis=1)
    both = jnp.concatenate([recur_map[...], input_map[...]], axis=1)
    swapped = pltpu.roll(both, GROUP, 1)
    left = lane < GROUP
    first = halves(jnp.where(left, both, 0.0), jnp.where(left, 0.0, swapped))
    second = halves(jnp.where(left, swapped, 0.0), jnp.where(left, 0.0, both))
    w_high, w_low = high_low(jnp.concatenate([first, second], axis=1))
    back_high, back_low = high_low(halves(jnp.transpose(first), jnp.transpose(second)))
    back_o[0] = back_high
    back_o[1] = back_low
    for p in range(8):
        at = slice(p * SPAN, (p + 1) * SPAN)
        far = slice((8 + p) * SPAN, (9 + p) * SPAN)
        b_s[pl.ds(24 + p, SPAN, stride=8), :] = jnp.transpose(
            halves(branch[:, at].astype(f32), branch[:, far].astype(f32))
        )
        fed_s[pl.ds(p, SPAN, stride=8), :] = jnp.transpose(
            halves(
                jnp.broadcast_to(shift[:, at], (GROUP, SPAN)), jnp.broadcast_to(shift[:, far], (GROUP, SPAN))
            )
        )
    for m in range(3):
        b_s[8 * m : 8 * m + 8, :] = before_of(b_s[1024 + 8 * m : 1032 + 8 * m, :])

    def gates(n, _):
        here = block_of(n)
        x = tiled(rows[0:1, :]) * b_s[here, :]
        for k in (1, 2, 3):
            x = x + tiled(rows[k : k + 1, :]) * b_s[moved_block(n, 8 * k), :]
        branch_o[here, :] = b_s[moved_block(n, 24), :].astype(bf16)
        x_high, x_low = high_low(x)
        pre = (
            jnp.dot(x_high, w_high, preferred_element_type=f32)
            + jnp.dot(x_low, w_high, preferred_element_type=f32)
            + jnp.dot(x_high, w_low, preferred_element_type=f32)
        )
        tr = jnp.tanh(0.5 * pre[:, :SPAN])
        ti = jnp.tanh(0.5 * pre[:, SPAN:])
        recur = 0.5 + 0.5 * tr
        inp = 0.5 + 0.5 * ti
        rate = tiled(rows[4:5, :])
        log = rate * recur + fed_s[here, :]
        decay = jnp.exp(log)
        square = decay * decay
        u = 2.0 * log
        series = -u * (1 + u * (1 / 2) * (1 + u * (1 / 3) * (1 + u * (1 / 4) * (1 + u * (1 / 5) * (1 + u * (1 / 6))))))
        left_over = jnp.where(u > -0.25, series, 1.0 - square)
        inverse = lax.rsqrt(left_over)
        root = left_over * inverse
        fed = inp * x
        pushed = root * fed
        decay_s[here, :] = decay
        fed_s[here, :] = pushed
        slope_s[here, :] = square * inverse * fed
        rate_s[here, :] = rate * (0.25 - 0.25 * tr * tr)
        recur_s[here, :] = recur
        c0_o[here, :] = (root * inp).astype(bf16)
        c1_o[here, :] = (pushed * (0.5 - 0.5 * ti)).astype(bf16)
        turned_o[:, here] = jnp.transpose(x).astype(bf16)
        return 0

    lax.fori_loop(0, 8, gates, 0)

    local_s[0:8, :] = jnp.zeros((8, SPAN), f32)
    power_s[0:8, :] = jnp.ones((8, SPAN), f32)

    def scan(n, held):
        value, power = held
        for m in range(8):
            at = pl.ds(pl.multiple_of(n * 64 + 8 * m, 8), 8)
            a = decay_s[at, :]
            value = fed_s[at, :] + a * value
            power = a * power
            to = pl.ds(pl.multiple_of(n * 64 + 8 * m + 8, 8), 8)
            local_s[to, :] = value
            power_s[to, :] = power
        return value, power

    value, power = lax.fori_loop(0, 16, scan, (jnp.zeros((8, SPAN), f32), jnp.ones((8, SPAN), f32)))
    enters = jnp.broadcast_to(entering(power, value, False)[None], (16, 8, SPAN)).reshape(SPAN, SPAN)

    def slopes(n, _):
        here = block_of(n)
        previous = local_s[here, :] + power_s[here, :] * enters
        decay = decay_s[here, :]
        slope = previous * decay - slope_s[here, :]
        c2_o[here, :] = (slope * rate_s[here, :]).astype(bf16)
        c3_o[here, :] = (slope * recur_s[here, :]).astype(bf16)
        fed_s[here, :] = local_s[moved_block(n, 8), :] + power_s[moved_block(n, 8), :] * enters
        return 0

    lax.fori_loop(0, 8, slopes, 0)
    next_o[0:1016, :] = decay_s[8:1024, :]
    next_o[1016:1024, :] = after_of(decay_s[0:8, :])
    for p in range(8):
        state = jnp.transpose(strided(fed_s, p))
        for half, at in ((0, slice(p * SPAN, (p + 1) * SPAN)), (1, slice((8 + p) * SPAN, (9 + p) * SPAN))):
            g = gate[:, at].astype(f32)
            c = 0.7978845608028654
            inner = jnp.tanh(c * (g + 0.044715 * (g * g * g)))
            part = 0.5 + 0.5 * inner
            turn = part + 0.5 * g * (1.0 - inner * inner) * (c * (1.0 + 3 * 0.044715 * (g * g)))
            g0_o[:, at] = (g * part).astype(bf16)
            g1_o[:, at] = (state[GROUP * half : GROUP * half + GROUP] * turn).astype(bf16)


def backward_kernel(
    cot, next_r, c0_r, c1_r, c2_r, c3_r, branch_r, turned_r, g0_r, g1_r, back_r, rows,
    gb_o, gate_o, small_o, d_s, local_s, power_s, dx_s, pushed_s,
):
    for p in range(8):
        parts = []
        for j in (p, 8 + p):
            at = slice(j * SPAN, (j + 1) * SPAN)
            c = cot[j].astype(f32)
            gate_o[:, at] = (c * g1_r[:, at].astype(f32)).astype(bf16)
            parts.append(c * g0_r[:, at].astype(f32))
        d_s[pl.ds(p, SPAN, stride=8), :] = jnp.transpose(halves(*parts))

    def scan(n, held):
        value, power = held
        for m in range(8):
            at = pl.ds(pl.multiple_of(1016 - n * 64 - 8 * m, 8), 8)
            a = next_r[at, :]
            value = d_s[at, :] + a * value
            power = a * power
            local_s[at, :] = value
            power_s[at, :] = power
        return value, power

    value, power = lax.fori_loop(0, 16, scan, (jnp.zeros((8, SPAN), f32), jnp.ones((8, SPAN), f32)))
    enters = jnp.broadcast_to(entering(power, value, True)[None], (16, 8, SPAN)).reshape(SPAN, SPAN)

    def summed(block):
        return jnp.sum(block.reshape(16, 8, SPAN), axis=0)

    def spread(n, total):
        here = block_of(n)
        grad = local_s[here, :] + power_s[here, :] * enters
        high = jnp.concatenate(
            [(grad * c2_r[here, :].astype(f32)).astype(bf16), (grad * c1_r[here, :].astype(f32)).astype(bf16)], axis=1
        )
        pushed_s[here, :] = high
        back = jnp.dot(high, back_r[0], preferred_element_type=f32) + jnp.dot(
            high, back_r[1], preferred_element_type=f32
        )
        dx_s[here, :] = grad * c0_r[here, :].astype(f32) + back
        return total + summed(grad * c3_r[here, :].astype(f32))

    zero = jnp.zeros((8, SPAN), f32)
    decays = lax.fori_loop(0, 8, spread, zero)
    for m in range(3):
        dx_s[1024 + 8 * m : 1032 + 8 * m, :] = after_of(dx_s[8 * m : 8 * m + 8, :])

    def taps(n, totals):
        here = block_of(n)
        value = branch_r[here, :].astype(f32)
        gb, out = None, []
        for k in range(CONV):
            dx = dx_s[moved_block(n, 8 * (3 - k)), :]
            term = tiled(rows[k : k + 1, :]) * dx
            gb = term if gb is None else gb + term
            out.append(totals[k] + summed(value * dx))
        d_s[here, :] = gb
        return tuple(out)

    totals = lax.fori_loop(0, 8, taps, (zero,) * CONV)
    for p in range(8):
        gb = jnp.transpose(strided(d_s, p)).astype(bf16)
        gb_o[p] = gb[:GROUP]
        gb_o[8 + p] = gb[GROUP:]
    product = jnp.dot(turned_r[...], pushed_s[...], preferred_element_type=f32)
    low = lanes((GROUP, SPAN)) < GROUP
    r_part = product[:GROUP, :SPAN] + pltpu.roll(product[GROUP:, :SPAN], GROUP, 1)
    i_part = pltpu.roll(product[:GROUP, SPAN:], GROUP, 1) + product[GROUP:, SPAN:]
    small_o[0:GROUP, :] = jnp.where(low, r_part, i_part).astype(bf16)
    row = lax.broadcasted_iota(jnp.int32, (8, SPAN), 0)
    table = zero
    for k, total in enumerate((*totals, decays * jnp.broadcast_to(rows[5:6, :], (8, SPAN)))):
        flat = jnp.broadcast_to(jnp.sum(total, axis=0, keepdims=True), (8, SPAN))
        table = jnp.where(row == k, flat + pltpu.roll(flat, GROUP, 1), table)
    small_o[GROUP : GROUP + 8, :] = table.astype(bf16)


VMEM = pl.BlockSpec(memory_space=pltpu.VMEM)
FLAT = (1024, SPAN)


def here_in_vmem(array):
    return pltpu.with_memory_space_constraint(array, pltpu.VMEM)


def forward_part(branch, gate, shift, conv, decay_param, recur_map, input_map):
    flat = jax.ShapeDtypeStruct(FLAT, bf16)
    plain = jax.ShapeDtypeStruct(branch.shape, bf16)
    return pl.pallas_call(
        forward_kernel,
        out_shape=[
            jax.ShapeDtypeStruct(FLAT, f32),
            *[flat] * 5,
            jax.ShapeDtypeStruct((SPAN, 1024), bf16),
            plain,
            plain,
            jax.ShapeDtypeStruct((2, 2 * SPAN, SPAN), bf16),
            jax.ShapeDtypeStruct((8, SPAN), f32),
        ],
        scratch_shapes=[pltpu.VMEM((1048, SPAN), f32)] + [pltpu.VMEM(FLAT, f32)] * 5 + [pltpu.VMEM((1032, SPAN), f32)] * 2,
        name="forward_part",
    )(branch, gate, shift, conv, decay_param, recur_map, input_map)


def backward_part(cot, saved):
    return pl.pallas_call(
        backward_kernel,
        out_shape=[
            jax.ShapeDtypeStruct((16, GROUP, SPAN), bf16),
            jax.ShapeDtypeStruct((GROUP, 2048), bf16),
            jax.ShapeDtypeStruct((GROUP + 8, 2 * GROUP), bf16),
        ],
        scratch_shapes=[pltpu.VMEM(FLAT, f32)] * 3 + [pltpu.VMEM((1048, SPAN), f32), pltpu.VMEM((1024, 2 * SPAN), bf16)],
        name="backward_part",
    )(cot, *saved)


def product_kernel(place, small, partner, own, near, far, grads, out):
    total = None
    blocks = (own[...], near[0:1024, :], far[0, 0:1024, :], far[1, 0:1024, :])
    for n, block in enumerate(blocks):
        theirs = grads[:, place[0] ^ NEAREST[n]].reshape(256, SPAN)
        term = lax.dot_general(block, theirs, (((1,), (1,)), ((), ())), preferred_element_type=f32)
        total = term if total is None else total + term
    pieces = out.shape[0]
    out[:, 0:32, :] = total.astype(bf16).reshape(pieces, 32, 256)
    mine = pl.ds(pl.multiple_of(place[2] * 32, 32), 32)
    maps = (small[mine, :].astype(f32) + partner[mine, :].astype(f32)).astype(bf16)
    rest = (small[64:72, :].astype(f32) + partner[64:72, :].astype(f32)).astype(bf16)
    top = jnp.concatenate([maps[0:16], maps[16:32]], axis=1)
    low = jnp.concatenate([rest, jnp.zeros((8, SPAN), bf16)], axis=1)
    out[:, 32:56, :] = jnp.broadcast_to(jnp.concatenate([top, low], axis=0)[None], (pieces, 24, 256))


def gather_sum_kernel(arrived, packed_o, conv_o, recur_o, input_o, decay_o):
    block = lax.broadcasted_iota(jnp.int32, (16, SPAN), 1) // 16
    totals = []
    for n in range(4):
        total = arrived[8 * n, 0:32, :].astype(f32)
        for m in range(1, 8):
            total = total + arrived[8 * n + m, 0:32, :].astype(f32)
        totals.append(total)
    for core in range(2):
        extra = arrived[core, 32:56, :].astype(f32)
        for n in range(core + 2, 32, 2):
            extra = extra + arrived[n, 32:56, :].astype(f32)
        for n in range(2):
            at = slice(32 * core + 16 * n, 32 * core + 16 * n + 16)
            half = extra[0:16, n * SPAN : (n + 1) * SPAN]
            recur_o[at, :] = half[:, 0:GROUP]
            input_o[at, :] = pltpu.roll(half, GROUP, 1)[:, 0:GROUP]
        if core == 0:
            conv_o[...] = extra[16:20, 0:GROUP]
            decay_o[...] = extra[20:21, 0:GROUP]
    for group in range(16):
        tile = slice((group // 8) * SPAN, (group // 8 + 1) * SPAN)
        piece = None
        for j in range(8):
            source = totals[j % 4][16 * (j // 4) : 16 * (j // 4) + 16, tile]
            shift = (16 * (j - group % 8)) % SPAN
            turned = pltpu.roll(source, shift, 1) if shift else source
            piece = turned if piece is None else jnp.where(block == j, turned, piece)
        packed_o[group] = piece.astype(bf16)


def last_sum_kernel(arrived, out):
    total = arrived[0].astype(f32)
    for n in range(1, arrived.shape[0]):
        total = total + arrived[n].astype(f32)
    out[0:16, :] = total[:, 0:GROUP]
    out[16:32, :] = pltpu.roll(total, GROUP, 1)[:, 0:GROUP]


def token_grad_kernel(place, proj, proj_other, own, one, two, three, out, tokens_s):
    for n, piece in enumerate((own, one, two, three)):
        tokens_s[:, place[0] ^ n] = piece[...]
    tokens = tokens_s[...].reshape(1024, SPAN)
    for k, half in enumerate((proj, proj_other)):
        tiles = half[...].reshape(16, 4, 8, 8, SPAN)
        result = None
        for n in range(8):
            term = jnp.dot(
                tiles[:, :, n].reshape(512, SPAN), tokens[n * SPAN : (n + 1) * SPAN], preferred_element_type=f32
            )
            result = term if result is None else result + term
        result = result.astype(bf16)
        for n in range(16):
            y, x = place[0] ^ NEAREST[n % 4], place[1] ^ NEAREST[n // 4]
            row = ((y * 4 + x) * 2 + (place[2] ^ k)) * 32
            out[pl.ds(pl.multiple_of(row, 32), 32), :] = result[32 * n : 32 * n + 32]


def exchanged(array, axis, bit):
    size = lax.axis_size(axis)
    return lax.ppermute(array, axis, [(n, n ^ bit) for n in range(size)])


def joined(array, axis, bits):
    return jnp.concatenate([array, exchanged(array, axis, bits)], axis=0)


def steps(
    normed, branch_in, gate_pre, cotangent, decay_shift,
    conv_weight, recur_weight, input_weight, decay_param, branch_proj,
):
    spans = lax.axis_size("sp")
    cot = lax.all_to_all(cotangent[0].reshape(spans, GROUP, SPAN), "sp", 0, 0, tiled=True)
    saved = forward_part(
        branch_in[0], gate_pre[0], decay_shift[0], conv_weight, decay_param[None], recur_weight[0], input_weight[0]
    )
    own = normed[0]
    width = branch_proj.shape[1] // SPAN
    rows = branch_proj.reshape(4, 8, width, SPAN).transpose(0, 2, 1, 3).reshape(-1, SPAN)
    packed = jnp.concatenate([own, rows], axis=0)
    near = exchanged(packed, "y", 1)
    far = exchanged(jnp.stack([packed, near]), "y", 3)
    held = jnp.stack([rows, near[1024:], far[0, 1024:], far[1, 1024:]])
    proj = joined(joined(held, "x", 1), "x", 3)
    proj_other = exchanged(proj, "core", 1)
    gb, grad_gate, small = backward_part(here_in_vmem(cot), [*map(here_in_vmem, saved[:5]), *saved[5:]])
    partner = exchanged(small, "core", 1)
    grads = lax.all_to_all(gb.reshape(64, 16, SPAN), ("sp", "y"), 0, 0, tiled=True)
    grads = grads.reshape(16, 4, 16, SPAN)
    here = lax.axis_index("y")
    place = jnp.stack([lax.axis_index(axis) for axis in DP]).astype(jnp.int32)
    smem = pl.BlockSpec(memory_space=pltpu.SMEM)
    pieces = pl.pallas_call(
        product_kernel,
        in_specs=[smem] + [VMEM] * 6,
        out_specs=VMEM,
        out_shape=jax.ShapeDtypeStruct((32, 56, 256), bf16),
        name="product",
    )(place, small, here_in_vmem(partner), own, near, here_in_vmem(far), here_in_vmem(grads))
    arrived = lax.all_to_all(pieces, DP, 0, 0, tiled=True)

    def part_for(n):
        return lax.dynamic_index_in_dim(grads, here ^ n, 1, keepdims=False)

    own_part = part_for(0)
    others = [exchanged(part_for(n), "y", n) for n in (1, 2, 3)]
    sums, grad_conv, grad_recur, grad_input, grad_decay = pl.pallas_call(
        gather_sum_kernel,
        out_shape=[
            jax.ShapeDtypeStruct((16, 16, SPAN), bf16),
            jax.ShapeDtypeStruct((CONV, GROUP), f32),
            jax.ShapeDtypeStruct((GROUP, GROUP), f32),
            jax.ShapeDtypeStruct((GROUP, GROUP), f32),
            jax.ShapeDtypeStruct((1, GROUP), f32),
        ],
        name="gather_sum",
    )(here_in_vmem(arrived))
    last = lax.all_to_all(sums, "sp", 0, 0, tiled=True)
    grad_proj = pl.pallas_call(
        last_sum_kernel, out_shape=jax.ShapeDtypeStruct((32, GROUP), f32), name="last_sum"
    )(here_in_vmem(last))
    grad_normed = pl.pallas_call(
        token_grad_kernel,
        in_specs=[smem] + [VMEM] * 6,
        out_specs=VMEM,
        out_shape=jax.ShapeDtypeStruct((1024, SPAN), bf16),
        scratch_shapes=[pltpu.VMEM((16, 4, 16, SPAN), bf16)],
        name="token_grad",
    )(place, proj, here_in_vmem(proj_other), *map(here_in_vmem, (own_part, *others)))
    return (
        grad_normed[None],
        grad_gate[None],
        grad_proj,
        grad_conv,
        grad_recur[None],
        grad_input[None],
        grad_decay[0],
    )


def solution(mesh):
    split = Mesh(mesh.devices.reshape(16, 4, 4, 2), ("sp", *DP))
    return jax.shard_map(
        steps,
        mesh=split,
        in_specs=(
            P(DP, None, "sp"),
            P(DP, "sp", None),
            P(DP, "sp", None),
            P(DP, None, "sp"),
            P(DP, "sp", None),
            P(None, "sp"),
            P("sp", None, None),
            P("sp", None, None),
            P("sp"),
            P(DP, None),
        ),
        out_specs=(
            P(DP, None, "sp"),
            P(DP, "sp", None),
            P(DP, "sp"),
            P(None, "sp"),
            P("sp", None, None),
            P("sp", None, None),
            P("sp"),
        ),
        check_vma=False,
    )
```

```python
import jax
import jax.numpy as jnp
from jax import lax
from jax.experimental import pallas as pl
from jax.experimental.pallas import tpu as pltpu
from jax.sharding import Mesh
from jax.sharding import PartitionSpec as P

SPAN = 128
GROUP = 64
CONV = 4
GATE = 8.0
f32 = jnp.float32
bf16 = jnp.bfloat16
DP = ("y", "x", "core")
NEAREST = (0, 1, 3, 2)


def lanes(shape):
    return lax.broadcasted_iota(jnp.int32, shape, 1)


def high_low(value):
    high = value.astype(bf16)
    return high, (value - high.astype(f32)).astype(bf16)


def strided(ref, n):
    return ref[pl.ds(n, SPAN, stride=8), :]


def before_of(block):
    row = lax.broadcasted_iota(jnp.int32, block.shape, 0)
    lane = lanes(block.shape)
    moved = pltpu.roll(block, 1, 0)
    across = jnp.where(lane >= GROUP, pltpu.roll(moved, GROUP, 1), 0.0)
    return jnp.where(row == 0, across, moved)


def after_of(block):
    row = lax.broadcasted_iota(jnp.int32, block.shape, 0)
    lane = lanes(block.shape)
    moved = pltpu.roll(block, 7, 0)
    across = jnp.where(lane < GROUP, pltpu.roll(moved, GROUP, 1), 0.0)
    return jnp.where(row == 7, across, moved)


def entering(factor, value, backward):
    row = lax.broadcasted_iota(jnp.int32, factor.shape, 0)
    lane = lanes(factor.shape)
    a, b = factor, value
    for step in (1, 2, 4):
        inside = row < 8 - step if backward else row >= step
        shift = 8 - step if backward else step
        b = b + a * jnp.where(inside, pltpu.roll(b, shift, 0), 0.0)
        a = a * jnp.where(inside, pltpu.roll(a, shift, 0), 1.0)
    edge = b[0:1] if backward else b[7:8]
    later = lane < GROUP if backward else lane >= GROUP
    base = jnp.where(later, jnp.broadcast_to(pltpu.roll(edge, GROUP, 1), factor.shape), 0.0)
    total = b + a * base
    return after_of(total) if backward else before_of(total)


def block_of(n):
    return pl.ds(pl.multiple_of(n * SPAN, SPAN), SPAN)


def moved_block(n, rows):
    return pl.ds(pl.multiple_of(n * SPAN + rows, 8), SPAN)


def tiled(row):
    return jnp.broadcast_to(row, (SPAN, SPAN))


def halves(top, low):
    return jnp.concatenate([top, low], axis=0)


def gelu_parts(g):
    c = 0.7978845608028654
    inner = jnp.tanh(c * (g + 0.044715 * (g * g * g)))
    part = 0.5 + 0.5 * inner
    return g * part, part + 0.5 * g * (1.0 - inner * inner) * (c * (1.0 + 3 * 0.044715 * (g * g)))


def forward_kernel(
    branch, gate, shift, conv, decay_param, recur_map, input_map,
    next_h, c0_h, c1_h, c2_h, c3_h, branch_h, turned_h, g0_h, state_h, back_o, rows,
    next_o, c0_o, c1_o, c2_o, c3_o, branch_o, turned_o, g0_o,
    b_s, decay_s, fed_s, slope_s, rate_s, recur_s, local_s, power_s, state_s, sems,
):
    copies = [
        pltpu.make_async_copy(source, target, sems.at[n])
        for n, (source, target) in enumerate(
            (
                (g0_o, g0_h), (next_o, next_h), (c0_o, c0_h), (c1_o, c1_h), (branch_o, branch_h),
                (turned_o, turned_h), (c2_o, c2_h), (c3_o, c3_h), (state_s, state_h),
            )
        )
    ]
    lane = lanes((GROUP, SPAN))
    g0_o[...] = gelu_parts(gate[...].astype(f32))[0].astype(bf16)
    copies[0].start()
    minus = -decay_param[...]
    softened = jnp.maximum(minus, 0.0) + jnp.log1p(jnp.exp(-jnp.abs(minus)))
    table = jnp.concatenate(
        [conv[...], -GATE * softened, GATE * (0.5 + 0.5 * jnp.tanh(0.5 * minus)), jnp.zeros((2, GROUP), f32)], axis=0
    )
    rows[...] = jnp.concatenate([table, table], axis=1)
    both = jnp.concatenate([recur_map[...], input_map[...]], axis=1)
    swapped = pltpu.roll(both, GROUP, 1)
    left = lane < GROUP
    first = halves(jnp.where(left, both, 0.0), jnp.where(left, 0.0, swapped))
    second = halves(jnp.where(left, swapped, 0.0), jnp.where(left, 0.0, both))
    w_high, w_low = high_low(jnp.concatenate([first, second], axis=1))
    back_high, back_low = high_low(halves(jnp.transpose(first), jnp.transpose(second)))
    back_o[0] = back_high
    back_o[1] = back_low
    wide = lanes((SPAN, SPAN)) < GROUP
    turned_shift = jnp.transpose(shift[...])
    for p in range(8):
        at = slice(p * SPAN, (p + 1) * SPAN)
        far = slice((8 + p) * SPAN, (9 + p) * SPAN)
        b_s[pl.ds(24 + p, SPAN, stride=8), :] = jnp.transpose(halves(branch[:, at], branch[:, far])).astype(f32)
        fed_s[pl.ds(p, SPAN, stride=8), :] = jnp.where(
            wide, tiled(turned_shift[:, p : p + 1]), tiled(turned_shift[:, 8 + p : 9 + p])
        )
    for m in range(3):
        b_s[8 * m : 8 * m + 8, :] = before_of(b_s[1024 + 8 * m : 1032 + 8 * m, :])

    def gates(n, _):
        here = block_of(n)
        x = tiled(rows[0:1, :]) * b_s[here, :]
        for k in (1, 2, 3):
            x = x + tiled(rows[k : k + 1, :]) * b_s[moved_block(n, 8 * k), :]
        branch_o[here, :] = b_s[moved_block(n, 24), :].astype(bf16)
        x_high, x_low = high_low(x)
        pre = (
            jnp.dot(x_high, w_high, preferred_element_type=f32)
            + jnp.dot(x_low, w_high, preferred_element_type=f32)
            + jnp.dot(x_high, w_low, preferred_element_type=f32)
        )
        tr = jnp.tanh(0.5 * pre[:, :SPAN])
        ti = jnp.tanh(0.5 * pre[:, SPAN:])
        recur = 0.5 + 0.5 * tr
        inp = 0.5 + 0.5 * ti
        rate = tiled(rows[4:5, :])
        log = rate * recur + fed_s[here, :]
        decay = jnp.exp(log)
        square = decay * decay
        u = 2.0 * log
        series = -u * (1 + u * (1 / 2) * (1 + u * (1 / 3) * (1 + u * (1 / 4) * (1 + u * (1 / 5) * (1 + u * (1 / 6))))))
        left_over = jnp.where(u > -0.25, series, 1.0 - square)
        inverse = lax.rsqrt(left_over)
        root = left_over * inverse
        fed = inp * x
        pushed = root * fed
        decay_s[here, :] = decay
        fed_s[here, :] = pushed
        slope_s[here, :] = square * inverse * fed
        rate_s[here, :] = rate * (0.25 - 0.25 * tr * tr)
        recur_s[here, :] = recur
        c0_o[here, :] = (root * inp).astype(bf16)
        c1_o[here, :] = (pushed * (0.5 - 0.5 * ti)).astype(bf16)
        turned_o[:, here] = jnp.transpose(x_high)
        return 0

    lax.fori_loop(0, 8, gates, 0, unroll=8)
    next_o[0:1016, :] = decay_s[8:1024, :]
    next_o[1016:1024, :] = after_of(decay_s[0:8, :])
    for copy in copies[1:6]:
        copy.start()
    local_s[0:8, :] = jnp.zeros((8, SPAN), f32)
    power_s[0:8, :] = jnp.ones((8, SPAN), f32)

    def scan(n, held):
        value, power = held
        for m in range(8):
            at = pl.ds(pl.multiple_of(n * 64 + 8 * m, 8), 8)
            a = decay_s[at, :]
            value = fed_s[at, :] + a * value
            power = a * power
            to = pl.ds(pl.multiple_of(n * 64 + 8 * m + 8, 8), 8)
            local_s[to, :] = value
            power_s[to, :] = power
        return value, power

    value, power = lax.fori_loop(0, 16, scan, (jnp.zeros((8, SPAN), f32), jnp.ones((8, SPAN), f32)))
    enters = jnp.broadcast_to(entering(power, value, False)[None], (16, 8, SPAN)).reshape(SPAN, SPAN)

    def slopes(n, _):
        here = block_of(n)
        previous = local_s[here, :] + power_s[here, :] * enters
        decay = decay_s[here, :]
        slope = previous * decay - slope_s[here, :]
        c2_o[here, :] = (slope * rate_s[here, :]).astype(bf16)
        c3_o[here, :] = (slope * recur_s[here, :]).astype(bf16)
        state_s[here, :] = local_s[moved_block(n, 8), :] + power_s[moved_block(n, 8), :] * enters
        return 0

    lax.fori_loop(0, 8, slopes, 0)
    for copy in copies[6:]:
        copy.start()
    for copy in copies:
        copy.wait()


def gate_kernel(cot, gate, state_r, gate_o):
    for p in range(8):
        state = jnp.transpose(strided(state_r, p))
        for half in range(2):
            j = 8 * half + p
            at = slice(j * SPAN, (j + 1) * SPAN)
            turn = gelu_parts(gate[:, at].astype(f32))[1]
            here = state[GROUP * half : GROUP * half + GROUP]
            gate_o[:, at] = (cot[j].astype(f32) * here * turn).astype(bf16)


def backward_kernel(
    cot, next_r, c0_r, c1_r, c2_r, c3_r, branch_r, turned_r, g0_r, back_r, rows,
    gb_o, small_o, d_s, local_s, power_s, dx_s, pushed_s,
):
    for p in range(8):
        parts = []
        for j in (p, 8 + p):
            at = slice(j * SPAN, (j + 1) * SPAN)
            c = cot[j].astype(f32)
            parts.append(c * g0_r[:, at].astype(f32))
        d_s[pl.ds(p, SPAN, stride=8), :] = jnp.transpose(halves(*parts))

    def scan(n, held):
        value, power = held
        for m in range(8):
            at = pl.ds(pl.multiple_of(1016 - n * 64 - 8 * m, 8), 8)
            a = next_r[at, :]
            value = d_s[at, :] + a * value
            power = a * power
            local_s[at, :] = value
            power_s[at, :] = power
        return value, power

    value, power = lax.fori_loop(0, 16, scan, (jnp.zeros((8, SPAN), f32), jnp.ones((8, SPAN), f32)))
    enters = jnp.broadcast_to(entering(power, value, True)[None], (16, 8, SPAN)).reshape(SPAN, SPAN)

    def summed(block):
        return jnp.sum(block.reshape(16, 8, SPAN), axis=0)

    def spread(n, total):
        here = block_of(n)
        grad = local_s[here, :] + power_s[here, :] * enters
        high = jnp.concatenate(
            [(grad * c2_r[here, :].astype(f32)).astype(bf16), (grad * c1_r[here, :].astype(f32)).astype(bf16)], axis=1
        )
        pushed_s[here, :] = high
        back = jnp.dot(high, back_r[0], preferred_element_type=f32) + jnp.dot(
            high, back_r[1], preferred_element_type=f32
        )
        dx_s[here, :] = grad * c0_r[here, :].astype(f32) + back
        return total + summed(grad * c3_r[here, :].astype(f32))

    zero = jnp.zeros((8, SPAN), f32)
    decays = lax.fori_loop(0, 8, spread, zero, unroll=8)
    for m in range(3):
        dx_s[1024 + 8 * m : 1032 + 8 * m, :] = after_of(dx_s[8 * m : 8 * m + 8, :])

    def taps(n, totals):
        here = block_of(n)
        value = branch_r[here, :].astype(f32)
        gb, out = None, []
        for k in range(CONV):
            dx = dx_s[moved_block(n, 8 * (3 - k)), :]
            term = tiled(rows[k : k + 1, :]) * dx
            gb = term if gb is None else gb + term
            out.append(totals[k] + summed(value * dx))
        d_s[here, :] = gb
        return tuple(out)

    totals = lax.fori_loop(0, 8, taps, (zero,) * CONV, unroll=8)
    for p in range(8):
        gb = jnp.transpose(strided(d_s, p)).astype(bf16)
        gb_o[p] = gb[:GROUP]
        gb_o[8 + p] = gb[GROUP:]
    product = jnp.dot(turned_r[...], pushed_s[...], preferred_element_type=f32)
    low = lanes((GROUP, SPAN)) < GROUP
    r_part = product[:GROUP, :SPAN] + pltpu.roll(product[GROUP:, :SPAN], GROUP, 1)
    i_part = pltpu.roll(product[:GROUP, SPAN:], GROUP, 1) + product[GROUP:, SPAN:]
    small_o[0:GROUP, :] = jnp.where(low, r_part, i_part).astype(bf16)
    row = lax.broadcasted_iota(jnp.int32, (8, SPAN), 0)
    table = zero
    for k, total in enumerate((*totals, decays * jnp.broadcast_to(rows[5:6, :], (8, SPAN)))):
        flat = jnp.broadcast_to(jnp.sum(total, axis=0, keepdims=True), (8, SPAN))
        table = jnp.where(row == k, flat + pltpu.roll(flat, GROUP, 1), table)
    small_o[GROUP : GROUP + 8, :] = table.astype(bf16)


VMEM = pl.BlockSpec(memory_space=pltpu.VMEM)
ANY = pl.BlockSpec(memory_space=pl.ANY)
FLAT = (1024, SPAN)


def here_in_vmem(array):
    return pltpu.with_memory_space_constraint(array, pltpu.VMEM)


def forward_part(branch, gate, shift, conv, decay_param, recur_map, input_map):
    flat = [(FLAT, f32)] + [(FLAT, bf16)] * 5 + [((SPAN, 1024), bf16), (branch.shape, bf16)]
    ends = [((2, 2 * SPAN, SPAN), bf16), ((8, SPAN), f32)]
    return pl.pallas_call(
        forward_kernel,
        in_specs=[VMEM] * 7,
        out_specs=[ANY] * 9 + [VMEM] * 2,
        out_shape=[jax.ShapeDtypeStruct(*each) for each in (*flat, (FLAT, f32), *ends)],
        scratch_shapes=[pltpu.VMEM(*each) for each in flat]
        + [pltpu.VMEM((1048, SPAN), f32)]
        + [pltpu.VMEM(FLAT, f32)] * 5
        + [pltpu.VMEM((1032, SPAN), f32)] * 2
        + [pltpu.VMEM(FLAT, f32), pltpu.SemaphoreType.DMA((9,))],
        name="forward_part",
    )(branch, gate, shift, conv, decay_param, recur_map, input_map)


def backward_part(cot, saved):
    return pl.pallas_call(
        backward_kernel,
        out_shape=[
            jax.ShapeDtypeStruct((16, GROUP, SPAN), bf16),
            jax.ShapeDtypeStruct((GROUP + 8, 2 * GROUP), bf16),
        ],
        scratch_shapes=[pltpu.VMEM(FLAT, f32)] * 3 + [pltpu.VMEM((1048, SPAN), f32), pltpu.VMEM((1024, 2 * SPAN), bf16)],
        name="backward_part",
    )(cot, *saved)


def gate_part(cot, gate, state):
    return pl.pallas_call(gate_kernel, out_shape=jax.ShapeDtypeStruct(gate.shape, bf16), name="gate_part")(
        cot, gate, state
    )


def product_kernel(place, small, partner, own, near, far, grads, out):
    total = None
    blocks = (own[...], near[0:1024, :], far[0, 0:1024, :], far[1, 0:1024, :])
    for n, block in enumerate(blocks):
        theirs = grads[:, place[0] ^ NEAREST[n]].reshape(256, SPAN)
        term = lax.dot_general(block, theirs, (((1,), (1,)), ((), ())), preferred_element_type=f32)
        total = term if total is None else total + term
    pieces = out.shape[0]
    out[:, 0:32, :] = total.astype(bf16).reshape(pieces, 32, 256)
    mine = pl.ds(pl.multiple_of(place[2] * 32, 32), 32)
    maps = (small[mine, :].astype(f32) + partner[mine, :].astype(f32)).astype(bf16)
    rest = (small[64:72, :].astype(f32) + partner[64:72, :].astype(f32)).astype(bf16)
    top = jnp.concatenate([maps[0:16], maps[16:32]], axis=1)
    low = jnp.concatenate([rest, jnp.zeros((8, SPAN), bf16)], axis=1)
    out[:, 32:56, :] = jnp.broadcast_to(jnp.concatenate([top, low], axis=0)[None], (pieces, 24, 256))


def gather_sum_kernel(arrived, packed_o, conv_o, recur_o, input_o, decay_o):
    block = lax.broadcasted_iota(jnp.int32, (16, SPAN), 1) // 16
    totals = []
    for n in range(4):
        total = arrived[8 * n, 0:32, :].astype(f32)
        for m in range(1, 8):
            total = total + arrived[8 * n + m, 0:32, :].astype(f32)
        totals.append(total)
    for core in range(2):
        extra = arrived[core, 32:56, :].astype(f32)
        for n in range(core + 2, 32, 2):
            extra = extra + arrived[n, 32:56, :].astype(f32)
        for n in range(2):
            at = slice(32 * core + 16 * n, 32 * core + 16 * n + 16)
            half = extra[0:16, n * SPAN : (n + 1) * SPAN]
            recur_o[at, :] = half[:, 0:GROUP]
            input_o[at, :] = pltpu.roll(half, GROUP, 1)[:, 0:GROUP]
        if core == 0:
            conv_o[...] = extra[16:20, 0:GROUP]
            decay_o[...] = extra[20:21, 0:GROUP]
    for group in range(16):
        tile = slice((group // 8) * SPAN, (group // 8 + 1) * SPAN)
        piece = None
        for j in range(8):
            source = totals[j % 4][16 * (j // 4) : 16 * (j // 4) + 16, tile]
            shift = (16 * (j - group % 8)) % SPAN
            turned = pltpu.roll(source, shift, 1) if shift else source
            piece = turned if piece is None else jnp.where(block == j, turned, piece)
        packed_o[group] = piece.astype(bf16)


def last_sum_kernel(arrived, out):
    total = arrived[0].astype(f32)
    for n in range(1, arrived.shape[0]):
        total = total + arrived[n].astype(f32)
    out[0:16, :] = total[:, 0:GROUP]
    out[16:32, :] = pltpu.roll(total, GROUP, 1)[:, 0:GROUP]


def token_grad_kernel(place, proj, proj_other, own, one, two, three, out, tokens_s):
    for n, piece in enumerate((own, one, two, three)):
        tokens_s[:, place[0] ^ n] = piece[...]
    tokens = tokens_s[...].reshape(1024, SPAN)
    for k, half in enumerate((proj, proj_other)):
        tiles = half[...].reshape(16, 4, 8, 8, SPAN)
        result = None
        for n in range(8):
            term = jnp.dot(
                tiles[:, :, n].reshape(512, SPAN), tokens[n * SPAN : (n + 1) * SPAN], preferred_element_type=f32
            )
            result = term if result is None else result + term
        result = result.astype(bf16)
        for n in range(16):
            y, x = place[0] ^ NEAREST[n % 4], place[1] ^ NEAREST[n // 4]
            row = ((y * 4 + x) * 2 + (place[2] ^ k)) * 32
            out[pl.ds(pl.multiple_of(row, 32), 32), :] = result[32 * n : 32 * n + 32]


def exchanged(array, axis, bit):
    size = lax.axis_size(axis)
    return lax.ppermute(array, axis, [(n, n ^ bit) for n in range(size)])


def joined(array, axis, bits):
    both = lax.optimization_barrier((array, exchanged(array, axis, bits)))
    return jnp.concatenate(both, axis=0)


def steps(
    normed, branch_in, gate_pre, cotangent, decay_shift,
    conv_weight, recur_weight, input_weight, decay_param, branch_proj,
):
    spans = lax.axis_size("sp")
    cot = lax.all_to_all(cotangent[0].reshape(spans, GROUP, SPAN), "sp", 0, 0, tiled=True)
    *saved, state, back_maps, taps = forward_part(
        here_in_vmem(branch_in[0]), here_in_vmem(gate_pre[0]), decay_shift.reshape(spans, SPAN),
        conv_weight, decay_param[None], recur_weight[0], input_weight[0],
    )
    saved = [*map(here_in_vmem, saved[:4]), *saved[4:], back_maps, taps]
    own = normed[0]
    width = branch_proj.shape[1] // SPAN
    rows = branch_proj.reshape(4, 8, width, SPAN).transpose(0, 2, 1, 3).reshape(-1, SPAN)
    packed = jnp.concatenate([own, rows], axis=0)
    near = exchanged(packed, "y", 1)
    far = exchanged(jnp.stack([packed, near]), "y", 3)
    held = jnp.stack([rows, near[1024:], far[0, 1024:], far[1, 1024:]])
    proj = joined(joined(held, "x", 1), "x", 3)
    proj_other = exchanged(proj, "core", 1)
    gb, small = backward_part(here_in_vmem(cot), saved)
    partner = exchanged(small, "core", 1)
    grads = lax.all_to_all(gb.reshape(64, 16, SPAN), ("sp", "y"), 0, 0, tiled=True)
    grads = grads.reshape(16, 4, 16, SPAN)
    here = lax.axis_index("y")
    place = jnp.stack([lax.axis_index(axis) for axis in DP]).astype(jnp.int32)
    smem = pl.BlockSpec(memory_space=pltpu.SMEM)
    pieces = pl.pallas_call(
        product_kernel,
        in_specs=[smem] + [VMEM] * 6,
        out_specs=VMEM,
        out_shape=jax.ShapeDtypeStruct((32, 56, 256), bf16),
        name="product",
    )(place, small, here_in_vmem(partner), own, near, far, here_in_vmem(grads))
    arrived = lax.all_to_all(pieces, DP, 0, 0, tiled=True)

    def part_for(n):
        return lax.dynamic_index_in_dim(grads, here ^ n, 1, keepdims=False)

    own_part = part_for(0)
    others = [exchanged(part_for(n), "y", n) for n in (1, 2, 3)]
    sums, grad_conv, grad_recur, grad_input, grad_decay = pl.pallas_call(
        gather_sum_kernel,
        out_shape=[
            jax.ShapeDtypeStruct((16, 16, SPAN), bf16),
            jax.ShapeDtypeStruct((CONV, GROUP), f32),
            jax.ShapeDtypeStruct((GROUP, GROUP), f32),
            jax.ShapeDtypeStruct((GROUP, GROUP), f32),
            jax.ShapeDtypeStruct((1, GROUP), f32),
        ],
        name="gather_sum",
    )(here_in_vmem(arrived))
    last = lax.all_to_all(sums, "sp", 0, 0, tiled=True)
    grad_proj = pl.pallas_call(
        last_sum_kernel, out_shape=jax.ShapeDtypeStruct((32, GROUP), f32), name="last_sum"
    )(here_in_vmem(last))
    grad_normed = pl.pallas_call(
        token_grad_kernel,
        in_specs=[smem] + [VMEM] * 6,
        out_specs=VMEM,
        out_shape=jax.ShapeDtypeStruct((1024, SPAN), bf16),
        scratch_shapes=[pltpu.VMEM((16, 4, 16, SPAN), bf16)],
        name="token_grad",
    )(place, proj, here_in_vmem(proj_other), *map(here_in_vmem, (own_part, *others)))
    grad_gate = gate_part(cot, gate_pre[0], state)
    return (
        grad_normed[None],
        grad_gate[None],
        grad_proj,
        grad_conv,
        grad_recur[None],
        grad_input[None],
        grad_decay[0],
    )


def solution(mesh):
    split = Mesh(mesh.devices.reshape(16, 4, 4, 2), ("sp", *DP))
    return jax.shard_map(
        steps,
        mesh=split,
        in_specs=(
            P(DP, None, "sp"),
            P(DP, "sp", None),
            P(DP, "sp", None),
            P(DP, None, "sp"),
            P(DP, "sp", None),
            P(None, "sp"),
            P("sp", None, None),
            P("sp", None, None),
            P("sp"),
            P(DP, None),
        ),
        out_specs=(
            P(DP, None, "sp"),
            P(DP, "sp", None),
            P(DP, "sp"),
            P(None, "sp"),
            P("sp", None, None),
            P("sp", None, None),
            P("sp"),
        ),
        check_vma=False,
    )
```

```python
import jax
import jax.numpy as jnp
from jax import lax
from jax.experimental import pallas as pl
from jax.experimental.pallas import tpu as pltpu
from jax.sharding import Mesh
from jax.sharding import PartitionSpec as P

SPAN = 128
GROUP = 64
CONV = 4
GATE = 8.0
f32 = jnp.float32
bf16 = jnp.bfloat16
DP = ("y", "x", "core")
NEAREST = (0, 1, 3, 2)


def lanes(shape):
    return lax.broadcasted_iota(jnp.int32, shape, 1)


def high_low(value):
    high = value.astype(bf16)
    return high, (value - high.astype(f32)).astype(bf16)


def strided(ref, n):
    return ref[pl.ds(n, SPAN, stride=8), :]


def before_of(block):
    row = lax.broadcasted_iota(jnp.int32, block.shape, 0)
    lane = lanes(block.shape)
    moved = pltpu.roll(block, 1, 0)
    across = jnp.where(lane >= GROUP, pltpu.roll(moved, GROUP, 1), 0.0)
    return jnp.where(row == 0, across, moved)


def after_of(block):
    row = lax.broadcasted_iota(jnp.int32, block.shape, 0)
    lane = lanes(block.shape)
    moved = pltpu.roll(block, 7, 0)
    across = jnp.where(lane < GROUP, pltpu.roll(moved, GROUP, 1), 0.0)
    return jnp.where(row == 7, across, moved)


def entering(factor, value, backward):
    row = lax.broadcasted_iota(jnp.int32, factor.shape, 0)
    lane = lanes(factor.shape)
    a, b = factor, value
    for step in (1, 2, 4):
        inside = row < 8 - step if backward else row >= step
        shift = 8 - step if backward else step
        b = b + a * jnp.where(inside, pltpu.roll(b, shift, 0), 0.0)
        a = a * jnp.where(inside, pltpu.roll(a, shift, 0), 1.0)
    edge = b[0:1] if backward else b[7:8]
    later = lane < GROUP if backward else lane >= GROUP
    base = jnp.where(later, jnp.broadcast_to(pltpu.roll(edge, GROUP, 1), factor.shape), 0.0)
    total = b + a * base
    return after_of(total) if backward else before_of(total)


def block_of(n):
    return pl.ds(pl.multiple_of(n * SPAN, SPAN), SPAN)


def moved_block(n, rows):
    return pl.ds(pl.multiple_of(n * SPAN + rows, 8), SPAN)


def tiled(row):
    return jnp.broadcast_to(row, (SPAN, SPAN))


def halves(top, low):
    return jnp.concatenate([top, low], axis=0)


def gelu_parts(g):
    c = 0.7978845608028654
    inner = jnp.tanh(c * (g + 0.044715 * (g * g * g)))
    part = 0.5 + 0.5 * inner
    return g * part, part + 0.5 * g * (1.0 - inner * inner) * (c * (1.0 + 3 * 0.044715 * (g * g)))


def forward_kernel(
    branch, gate, shift, conv, decay_param, recur_map, input_map,
    next_h, c0_h, c1_h, c2_h, c3_h, branch_h, turned_h, g0_h, g1_h, back_o, rows,
    next_o, c0_o, c1_o, c2_o, c3_o, branch_o, turned_o, g0_o, g1_o,
    b_s, decay_s, fed_s, slope_s, rate_s, recur_s, local_s, power_s, state_s, sems,
):
    copies = [
        pltpu.make_async_copy(source, target, sems.at[n])
        for n, (source, target) in enumerate(
            (
                (g0_o, g0_h), (next_o, next_h), (c0_o, c0_h), (c1_o, c1_h), (branch_o, branch_h),
                (turned_o, turned_h), (c2_o, c2_h), (c3_o, c3_h), (g1_o, g1_h),
            )
        )
    ]
    lane = lanes((GROUP, SPAN))
    g0_o[...] = gelu_parts(gate[...].astype(f32))[0].astype(bf16)
    copies[0].start()
    minus = -decay_param[...]
    softened = jnp.maximum(minus, 0.0) + jnp.log1p(jnp.exp(-jnp.abs(minus)))
    table = jnp.concatenate(
        [conv[...], -GATE * softened, GATE * (0.5 + 0.5 * jnp.tanh(0.5 * minus)), jnp.zeros((2, GROUP), f32)], axis=0
    )
    rows[...] = jnp.concatenate([table, table], axis=1)
    both = jnp.concatenate([recur_map[...], input_map[...]], axis=1)
    swapped = pltpu.roll(both, GROUP, 1)
    left = lane < GROUP
    first = halves(jnp.where(left, both, 0.0), jnp.where(left, 0.0, swapped))
    second = halves(jnp.where(left, swapped, 0.0), jnp.where(left, 0.0, both))
    w_high, w_low = high_low(jnp.concatenate([first, second], axis=1))
    back_high, back_low = high_low(halves(jnp.transpose(first), jnp.transpose(second)))
    back_o[0] = back_high
    back_o[1] = back_low
    wide = lanes((SPAN, SPAN)) < GROUP
    turned_shift = jnp.transpose(shift[...])
    for p in range(8):
        at = slice(p * SPAN, (p + 1) * SPAN)
        far = slice((8 + p) * SPAN, (9 + p) * SPAN)
        b_s[pl.ds(24 + p, SPAN, stride=8), :] = jnp.transpose(halves(branch[:, at], branch[:, far])).astype(f32)
        fed_s[pl.ds(p, SPAN, stride=8), :] = jnp.where(
            wide, tiled(turned_shift[:, p : p + 1]), tiled(turned_shift[:, 8 + p : 9 + p])
        )
    for m in range(3):
        b_s[8 * m : 8 * m + 8, :] = before_of(b_s[1024 + 8 * m : 1032 + 8 * m, :])

    def gates(n, _):
        here = block_of(n)
        x = tiled(rows[0:1, :]) * b_s[here, :]
        for k in (1, 2, 3):
            x = x + tiled(rows[k : k + 1, :]) * b_s[moved_block(n, 8 * k), :]
        branch_o[here, :] = b_s[moved_block(n, 24), :].astype(bf16)
        x_high, x_low = high_low(x)
        pre = (
            jnp.dot(x_high, w_high, preferred_element_type=f32)
            + jnp.dot(x_low, w_high, preferred_element_type=f32)
            + jnp.dot(x_high, w_low, preferred_element_type=f32)
        )
        tr = jnp.tanh(0.5 * pre[:, :SPAN])
        ti = jnp.tanh(0.5 * pre[:, SPAN:])
        recur = 0.5 + 0.5 * tr
        inp = 0.5 + 0.5 * ti
        rate = tiled(rows[4:5, :])
        log = rate * recur + fed_s[here, :]
        decay = jnp.exp(log)
        square = decay * decay
        u = 2.0 * log
        series = -u * (1 + u * (1 / 2) * (1 + u * (1 / 3) * (1 + u * (1 / 4) * (1 + u * (1 / 5) * (1 + u * (1 / 6))))))
        left_over = jnp.where(u > -0.25, series, 1.0 - square)
        inverse = lax.rsqrt(left_over)
        root = left_over * inverse
        fed = inp * x
        pushed = root * fed
        decay_s[here, :] = decay
        fed_s[here, :] = pushed
        slope_s[here, :] = square * inverse * fed
        rate_s[here, :] = rate * (0.25 - 0.25 * tr * tr)
        recur_s[here, :] = recur
        c0_o[here, :] = (root * inp).astype(bf16)
        c1_o[here, :] = (pushed * (0.5 - 0.5 * ti)).astype(bf16)
        turned_o[:, here] = jnp.transpose(x_high)
        return 0

    lax.fori_loop(0, 8, gates, 0, unroll=8)
    next_o[0:1016, :] = decay_s[8:1024, :]
    next_o[1016:1024, :] = after_of(decay_s[0:8, :])
    for copy in copies[1:6]:
        copy.start()
    local_s[0:8, :] = jnp.zeros((8, SPAN), f32)
    power_s[0:8, :] = jnp.ones((8, SPAN), f32)

    def scan(n, held):
        value, power = held
        for m in range(8):
            at = pl.ds(pl.multiple_of(n * 64 + 8 * m, 8), 8)
            a = decay_s[at, :]
            value = fed_s[at, :] + a * value
            power = a * power
            to = pl.ds(pl.multiple_of(n * 64 + 8 * m + 8, 8), 8)
            local_s[to, :] = value
            power_s[to, :] = power
        return value, power

    value, power = lax.fori_loop(0, 16, scan, (jnp.zeros((8, SPAN), f32), jnp.ones((8, SPAN), f32)))
    enters = jnp.broadcast_to(entering(power, value, False)[None], (16, 8, SPAN)).reshape(SPAN, SPAN)

    def slopes(n, _):
        here = block_of(n)
        previous = local_s[here, :] + power_s[here, :] * enters
        decay = decay_s[here, :]
        slope = previous * decay - slope_s[here, :]
        c2_o[here, :] = (slope * rate_s[here, :]).astype(bf16)
        c3_o[here, :] = (slope * recur_s[here, :]).astype(bf16)
        state_s[here, :] = local_s[moved_block(n, 8), :] + power_s[moved_block(n, 8), :] * enters
        return 0

    lax.fori_loop(0, 8, slopes, 0)
    for copy in copies[6:8]:
        copy.start()
    for p in range(8):
        state = jnp.transpose(strided(state_s, p))
        for half in range(2):
            at = slice((8 * half + p) * SPAN, (8 * half + p + 1) * SPAN)
            turn = gelu_parts(gate[:, at].astype(f32))[1]
            g1_o[:, at] = (state[GROUP * half : GROUP * half + GROUP] * turn).astype(bf16)
    copies[8].start()
    for copy in copies:
        copy.wait()


def backward_kernel(
    cot, next_r, c0_r, c1_r, c2_r, c3_r, branch_r, turned_r, g0_r, back_r, rows,
    gb_o, small_o, d_s, local_s, power_s, dx_s, pushed_s,
):
    for p in range(8):
        parts = []
        for j in (p, 8 + p):
            at = slice(j * SPAN, (j + 1) * SPAN)
            c = cot[j].astype(f32)
            parts.append(c * g0_r[:, at].astype(f32))
        d_s[pl.ds(p, SPAN, stride=8), :] = jnp.transpose(halves(*parts))

    def scan(n, held):
        value, power = held
        for m in range(8):
            at = pl.ds(pl.multiple_of(1016 - n * 64 - 8 * m, 8), 8)
            a = next_r[at, :]
            value = d_s[at, :] + a * value
            power = a * power
            local_s[at, :] = value
            power_s[at, :] = power
        return value, power

    value, power = lax.fori_loop(0, 16, scan, (jnp.zeros((8, SPAN), f32), jnp.ones((8, SPAN), f32)))
    enters = jnp.broadcast_to(entering(power, value, True)[None], (16, 8, SPAN)).reshape(SPAN, SPAN)

    def summed(block):
        return jnp.sum(block.reshape(16, 8, SPAN), axis=0)

    def spread(n, total):
        here = block_of(n)
        grad = local_s[here, :] + power_s[here, :] * enters
        high = jnp.concatenate(
            [(grad * c2_r[here, :].astype(f32)).astype(bf16), (grad * c1_r[here, :].astype(f32)).astype(bf16)], axis=1
        )
        pushed_s[here, :] = high
        back = jnp.dot(high, back_r[0], preferred_element_type=f32) + jnp.dot(
            high, back_r[1], preferred_element_type=f32
        )
        dx_s[here, :] = grad * c0_r[here, :].astype(f32) + back
        return total + summed(grad * c3_r[here, :].astype(f32))

    zero = jnp.zeros((8, SPAN), f32)
    decays = lax.fori_loop(0, 8, spread, zero, unroll=8)
    for m in range(3):
        dx_s[1024 + 8 * m : 1032 + 8 * m, :] = after_of(dx_s[8 * m : 8 * m + 8, :])

    def taps(n, totals):
        here = block_of(n)
        value = branch_r[here, :].astype(f32)
        gb, out = None, []
        for k in range(CONV):
            dx = dx_s[moved_block(n, 8 * (3 - k)), :]
            term = tiled(rows[k : k + 1, :]) * dx
            gb = term if gb is None else gb + term
            out.append(totals[k] + summed(value * dx))
        d_s[here, :] = gb
        return tuple(out)

    totals = lax.fori_loop(0, 8, taps, (zero,) * CONV, unroll=8)
    for p in range(8):
        gb = jnp.transpose(strided(d_s, p)).astype(bf16)
        gb_o[p] = gb[:GROUP]
        gb_o[8 + p] = gb[GROUP:]
    product = jnp.dot(turned_r[...], pushed_s[...], preferred_element_type=f32)
    low = lanes((GROUP, SPAN)) < GROUP
    r_part = product[:GROUP, :SPAN] + pltpu.roll(product[GROUP:, :SPAN], GROUP, 1)
    i_part = pltpu.roll(product[:GROUP, SPAN:], GROUP, 1) + product[GROUP:, SPAN:]
    small_o[0:GROUP, :] = jnp.where(low, r_part, i_part).astype(bf16)
    row = lax.broadcasted_iota(jnp.int32, (8, SPAN), 0)
    table = zero
    for k, total in enumerate((*totals, decays * jnp.broadcast_to(rows[5:6, :], (8, SPAN)))):
        flat = jnp.broadcast_to(jnp.sum(total, axis=0, keepdims=True), (8, SPAN))
        table = jnp.where(row == k, flat + pltpu.roll(flat, GROUP, 1), table)
    small_o[GROUP : GROUP + 8, :] = table.astype(bf16)


VMEM = pl.BlockSpec(memory_space=pltpu.VMEM)
ANY = pl.BlockSpec(memory_space=pl.ANY)
FLAT = (1024, SPAN)


def here_in_vmem(array):
    return pltpu.with_memory_space_constraint(array, pltpu.VMEM)


def forward_part(branch, gate, shift, conv, decay_param, recur_map, input_map):
    flat = [(FLAT, f32)] + [(FLAT, bf16)] * 5 + [((SPAN, 1024), bf16)] + [(branch.shape, bf16)] * 2
    ends = [((2, 2 * SPAN, SPAN), bf16), ((8, SPAN), f32)]
    return pl.pallas_call(
        forward_kernel,
        in_specs=[VMEM] * 7,
        out_specs=[ANY] * 9 + [VMEM] * 2,
        out_shape=[jax.ShapeDtypeStruct(*each) for each in (*flat, *ends)],
        scratch_shapes=[pltpu.VMEM(*each) for each in flat]
        + [pltpu.VMEM((1048, SPAN), f32)]
        + [pltpu.VMEM(FLAT, f32)] * 5
        + [pltpu.VMEM((1032, SPAN), f32)] * 2
        + [pltpu.VMEM(FLAT, f32), pltpu.SemaphoreType.DMA((9,))],
        name="forward_part",
    )(branch, gate, shift, conv, decay_param, recur_map, input_map)


def backward_part(cot, saved):
    return pl.pallas_call(
        backward_kernel,
        out_shape=[
            jax.ShapeDtypeStruct((16, GROUP, SPAN), bf16),
            jax.ShapeDtypeStruct((GROUP + 8, 2 * GROUP), bf16),
        ],
        scratch_shapes=[pltpu.VMEM(FLAT, f32)] * 3 + [pltpu.VMEM((1048, SPAN), f32), pltpu.VMEM((1024, 2 * SPAN), bf16)],
        name="backward_part",
    )(cot, *saved)


def product_kernel(place, small, partner, own, near, far, grads, out):
    total = None
    blocks = (own[...], near[0:1024, :], far[0, 0:1024, :], far[1, 0:1024, :])
    for n, block in enumerate(blocks):
        theirs = grads[:, place[0] ^ NEAREST[n]].reshape(256, SPAN)
        term = lax.dot_general(block, theirs, (((1,), (1,)), ((), ())), preferred_element_type=f32)
        total = term if total is None else total + term
    pieces = out.shape[0]
    out[:, 0:32, :] = total.astype(bf16).reshape(pieces, 32, 256)
    mine = pl.ds(pl.multiple_of(place[2] * 32, 32), 32)
    maps = (small[mine, :].astype(f32) + partner[mine, :].astype(f32)).astype(bf16)
    rest = (small[64:72, :].astype(f32) + partner[64:72, :].astype(f32)).astype(bf16)
    top = jnp.concatenate([maps[0:16], maps[16:32]], axis=1)
    low = jnp.concatenate([rest, jnp.zeros((8, SPAN), bf16)], axis=1)
    out[:, 32:56, :] = jnp.broadcast_to(jnp.concatenate([top, low], axis=0)[None], (pieces, 24, 256))


def gather_sum_kernel(arrived, packed_o, conv_o, recur_o, input_o, decay_o):
    block = lax.broadcasted_iota(jnp.int32, (16, SPAN), 1) // 16
    totals = []
    for n in range(4):
        total = arrived[8 * n, 0:32, :].astype(f32)
        for m in range(1, 8):
            total = total + arrived[8 * n + m, 0:32, :].astype(f32)
        totals.append(total)
    for core in range(2):
        extra = arrived[core, 32:56, :].astype(f32)
        for n in range(core + 2, 32, 2):
            extra = extra + arrived[n, 32:56, :].astype(f32)
        for n in range(2):
            at = slice(32 * core + 16 * n, 32 * core + 16 * n + 16)
            half = extra[0:16, n * SPAN : (n + 1) * SPAN]
            recur_o[at, :] = half[:, 0:GROUP]
            input_o[at, :] = pltpu.roll(half, GROUP, 1)[:, 0:GROUP]
        if core == 0:
            conv_o[...] = extra[16:20, 0:GROUP]
            decay_o[...] = extra[20:21, 0:GROUP]
    for group in range(16):
        tile = slice((group // 8) * SPAN, (group // 8 + 1) * SPAN)
        piece = None
        for j in range(8):
            source = totals[j % 4][16 * (j // 4) : 16 * (j // 4) + 16, tile]
            shift = (16 * (j - group % 8)) % SPAN
            turned = pltpu.roll(source, shift, 1) if shift else source
            piece = turned if piece is None else jnp.where(block == j, turned, piece)
        packed_o[group] = piece.astype(bf16)


def last_sum_kernel(arrived, out):
    total = arrived[0].astype(f32)
    for n in range(1, arrived.shape[0]):
        total = total + arrived[n].astype(f32)
    out[0:16, :] = total[:, 0:GROUP]
    out[16:32, :] = pltpu.roll(total, GROUP, 1)[:, 0:GROUP]


def token_grad_kernel(place, proj, proj_other, own, one, two, three, cot, g1, out, gate_o, tokens_s):
    for j in range(cot.shape[0]):
        at = slice(j * SPAN, (j + 1) * SPAN)
        gate_o[:, at] = (cot[j].astype(f32) * g1[:, at].astype(f32)).astype(bf16)
    for n, piece in enumerate((own, one, two, three)):
        tokens_s[:, place[0] ^ n] = piece[...]
    tokens = tokens_s[...].reshape(1024, SPAN)
    for k, half in enumerate((proj, proj_other)):
        tiles = half[...].reshape(16, 4, 8, 8, SPAN)
        result = None
        for n in range(8):
            term = jnp.dot(
                tiles[:, :, n].reshape(512, SPAN), tokens[n * SPAN : (n + 1) * SPAN], preferred_element_type=f32
            )
            result = term if result is None else result + term
        result = result.astype(bf16)
        for n in range(16):
            y, x = place[0] ^ NEAREST[n % 4], place[1] ^ NEAREST[n // 4]
            row = ((y * 4 + x) * 2 + (place[2] ^ k)) * 32
            out[pl.ds(pl.multiple_of(row, 32), 32), :] = result[32 * n : 32 * n + 32]


def exchanged(array, axis, bit):
    size = lax.axis_size(axis)
    return lax.ppermute(array, axis, [(n, n ^ bit) for n in range(size)])


def joined(array, axis, bits):
    both = lax.optimization_barrier((array, exchanged(array, axis, bits)))
    return jnp.concatenate(both, axis=0)


def steps(
    normed, branch_in, gate_pre, cotangent, decay_shift,
    conv_weight, recur_weight, input_weight, decay_param, branch_proj,
):
    spans = lax.axis_size("sp")
    cot = lax.all_to_all(cotangent[0].reshape(spans, GROUP, SPAN), "sp", 0, 0, tiled=True)
    *saved, g1, back_maps, taps = forward_part(
        here_in_vmem(branch_in[0]), here_in_vmem(gate_pre[0]), decay_shift.reshape(spans, SPAN),
        conv_weight, decay_param[None], recur_weight[0], input_weight[0],
    )
    saved = [*map(here_in_vmem, saved[:4]), *saved[4:], back_maps, taps]
    own = normed[0]
    width = branch_proj.shape[1] // SPAN
    rows = branch_proj.reshape(4, 8, width, SPAN).transpose(0, 2, 1, 3).reshape(-1, SPAN)
    packed = jnp.concatenate([own, rows], axis=0)
    near = exchanged(packed, "y", 1)
    far = exchanged(jnp.stack([packed, near]), "y", 3)
    held = jnp.stack([rows, near[1024:], far[0, 1024:], far[1, 1024:]])
    proj = joined(joined(held, "x", 1), "x", 3)
    proj_other = exchanged(proj, "core", 1)
    gb, small = backward_part(here_in_vmem(cot), saved)
    partner = exchanged(small, "core", 1)
    grads = lax.all_to_all(gb.reshape(64, 16, SPAN), ("sp", "y"), 0, 0, tiled=True)
    grads = grads.reshape(16, 4, 16, SPAN)
    here = lax.axis_index("y")
    place = jnp.stack([lax.axis_index(axis) for axis in DP]).astype(jnp.int32)
    smem = pl.BlockSpec(memory_space=pltpu.SMEM)
    pieces = pl.pallas_call(
        product_kernel,
        in_specs=[smem] + [VMEM] * 6,
        out_specs=VMEM,
        out_shape=jax.ShapeDtypeStruct((32, 56, 256), bf16),
        name="product",
    )(place, small, here_in_vmem(partner), own, here_in_vmem(near), here_in_vmem(far), here_in_vmem(grads))
    arrived = lax.all_to_all(pieces, DP, 0, 0, tiled=True)

    def part_for(n):
        return lax.dynamic_index_in_dim(grads, here ^ n, 1, keepdims=False)

    own_part = part_for(0)
    others = [exchanged(part_for(n), "y", n) for n in (1, 2, 3)]
    sums, grad_conv, grad_recur, grad_input, grad_decay = pl.pallas_call(
        gather_sum_kernel,
        out_shape=[
            jax.ShapeDtypeStruct((16, 16, SPAN), bf16),
            jax.ShapeDtypeStruct((CONV, GROUP), f32),
            jax.ShapeDtypeStruct((GROUP, GROUP), f32),
            jax.ShapeDtypeStruct((GROUP, GROUP), f32),
            jax.ShapeDtypeStruct((1, GROUP), f32),
        ],
        name="gather_sum",
    )(here_in_vmem(arrived))
    last = lax.all_to_all(sums, "sp", 0, 0, tiled=True)
    grad_proj = pl.pallas_call(
        last_sum_kernel, out_shape=jax.ShapeDtypeStruct((32, GROUP), f32), name="last_sum"
    )(here_in_vmem(last))
    grad_normed, grad_gate = pl.pallas_call(
        token_grad_kernel,
        in_specs=[smem] + [VMEM] * 8,
        out_specs=[VMEM] * 2,
        out_shape=[jax.ShapeDtypeStruct((1024, SPAN), bf16), jax.ShapeDtypeStruct(g1.shape, bf16)],
        scratch_shapes=[pltpu.VMEM((16, 4, 16, SPAN), bf16)],
        name="token_grad",
    )(place, proj, here_in_vmem(proj_other), *map(here_in_vmem, (own_part, *others)), cot, g1)
    return (
        grad_normed[None],
        grad_gate[None],
        grad_proj,
        grad_conv,
        grad_recur[None],
        grad_input[None],
        grad_decay[0],
    )


def solution(mesh):
    split = Mesh(mesh.devices.reshape(16, 4, 4, 2), ("sp", *DP))
    return jax.shard_map(
        steps,
        mesh=split,
        in_specs=(
            P(DP, None, "sp"),
            P(DP, "sp", None),
            P(DP, "sp", None),
            P(DP, None, "sp"),
            P(DP, "sp", None),
            P(None, "sp"),
            P("sp", None, None),
            P("sp", None, None),
            P("sp"),
            P(DP, None),
        ),
        out_specs=(
            P(DP, None, "sp"),
            P(DP, "sp", None),
            P(DP, "sp"),
            P(None, "sp"),
            P("sp", None, None),
            P("sp", None, None),
            P("sp"),
        ),
        check_vma=False,
    )
```

```python
import jax
import jax.numpy as jnp
from jax import lax
from jax.experimental import pallas as pl
from jax.experimental.pallas import tpu as pltpu
from jax.sharding import Mesh
from jax.sharding import PartitionSpec as P

SPAN = 128
GROUP = 64
CONV = 4
GATE = 8.0
f32 = jnp.float32
bf16 = jnp.bfloat16
DP = ("y", "x", "core")
NEAREST = (0, 1, 3, 2)


def lanes(shape):
    return lax.broadcasted_iota(jnp.int32, shape, 1)


def high_low(value):
    high = value.astype(bf16)
    return high, (value - high.astype(f32)).astype(bf16)


def strided(ref, n):
    return ref[pl.ds(n, SPAN, stride=8), :]


def before_of(block):
    row = lax.broadcasted_iota(jnp.int32, block.shape, 0)
    lane = lanes(block.shape)
    moved = pltpu.roll(block, 1, 0)
    across = jnp.where(lane >= GROUP, pltpu.roll(moved, GROUP, 1), 0.0)
    return jnp.where(row == 0, across, moved)


def after_of(block):
    row = lax.broadcasted_iota(jnp.int32, block.shape, 0)
    lane = lanes(block.shape)
    moved = pltpu.roll(block, 7, 0)
    across = jnp.where(lane < GROUP, pltpu.roll(moved, GROUP, 1), 0.0)
    return jnp.where(row == 7, across, moved)


def entering(factor, value, backward):
    row = lax.broadcasted_iota(jnp.int32, factor.shape, 0)
    lane = lanes(factor.shape)
    a, b = factor, value
    for step in (1, 2, 4):
        inside = row < 8 - step if backward else row >= step
        shift = 8 - step if backward else step
        b = b + a * jnp.where(inside, pltpu.roll(b, shift, 0), 0.0)
        a = a * jnp.where(inside, pltpu.roll(a, shift, 0), 1.0)
    edge = b[0:1] if backward else b[7:8]
    later = lane < GROUP if backward else lane >= GROUP
    base = jnp.where(later, jnp.broadcast_to(pltpu.roll(edge, GROUP, 1), factor.shape), 0.0)
    total = b + a * base
    return after_of(total) if backward else before_of(total)


def block_of(n):
    return pl.ds(pl.multiple_of(n * SPAN, SPAN), SPAN)


def moved_block(n, rows):
    return pl.ds(pl.multiple_of(n * SPAN + rows, 8), SPAN)


def tiled(row):
    return jnp.broadcast_to(row, (SPAN, SPAN))


def halves(top, low):
    return jnp.concatenate([top, low], axis=0)


def gelu_parts(g):
    c = 0.7978845608028654
    inner = jnp.tanh(c * (g + 0.044715 * (g * g * g)))
    part = 0.5 + 0.5 * inner
    return g * part, part + 0.5 * g * (1.0 - inner * inner) * (c * (1.0 + 3 * 0.044715 * (g * g)))


def forward_kernel(
    branch, gate, shift, conv, decay_param, recur_map, input_map,
    next_h, c0_h, c1_h, c2_h, c3_h, branch_h, turned_h, g0_h, g1_h, back_o, rows,
    next_o, c0_o, c1_o, c2_o, c3_o, branch_o, turned_o, g0_o, g1_o,
    b_s, decay_s, fed_s, slope_s, rate_s, recur_s, local_s, power_s, state_s, sems,
):
    copies = [
        pltpu.make_async_copy(source, target, sems.at[n])
        for n, (source, target) in enumerate(
            (
                (g0_o, g0_h), (next_o, next_h), (c0_o, c0_h), (c1_o, c1_h), (branch_o, branch_h),
                (turned_o, turned_h), (c2_o, c2_h), (c3_o, c3_h), (g1_o, g1_h),
            )
        )
    ]
    lane = lanes((GROUP, SPAN))
    g0_o[...] = gelu_parts(gate[...].astype(f32))[0].astype(bf16)
    copies[0].start()
    minus = -decay_param[...]
    softened = jnp.maximum(minus, 0.0) + jnp.log1p(jnp.exp(-jnp.abs(minus)))
    table = jnp.concatenate(
        [conv[...], -GATE * softened, GATE * (0.5 + 0.5 * jnp.tanh(0.5 * minus)), jnp.zeros((2, GROUP), f32)], axis=0
    )
    rows[...] = jnp.concatenate([table, table], axis=1)
    both = jnp.concatenate([recur_map[...], input_map[...]], axis=1)
    swapped = pltpu.roll(both, GROUP, 1)
    left = lane < GROUP
    first = halves(jnp.where(left, both, 0.0), jnp.where(left, 0.0, swapped))
    second = halves(jnp.where(left, swapped, 0.0), jnp.where(left, 0.0, both))
    w_high, w_low = high_low(jnp.concatenate([first, second], axis=1))
    back_high, back_low = high_low(halves(jnp.transpose(first), jnp.transpose(second)))
    back_o[0] = back_high
    back_o[1] = back_low
    wide = lanes((SPAN, SPAN)) < GROUP
    turned_shift = jnp.transpose(shift[...])
    for p in range(8):
        at = slice(p * SPAN, (p + 1) * SPAN)
        far = slice((8 + p) * SPAN, (9 + p) * SPAN)
        b_s[pl.ds(24 + p, SPAN, stride=8), :] = jnp.transpose(halves(branch[:, at], branch[:, far])).astype(f32)
        fed_s[pl.ds(p, SPAN, stride=8), :] = jnp.where(
            wide, tiled(turned_shift[:, p : p + 1]), tiled(turned_shift[:, 8 + p : 9 + p])
        )
    for m in range(3):
        b_s[8 * m : 8 * m + 8, :] = before_of(b_s[1024 + 8 * m : 1032 + 8 * m, :])

    def gates(n, _):
        here = block_of(n)
        x = tiled(rows[0:1, :]) * b_s[here, :]
        for k in (1, 2, 3):
            x = x + tiled(rows[k : k + 1, :]) * b_s[moved_block(n, 8 * k), :]
        branch_o[here, :] = b_s[moved_block(n, 24), :].astype(bf16)
        x_high, x_low = high_low(x)
        pre = (
            jnp.dot(x_high, w_high, preferred_element_type=f32)
            + jnp.dot(x_low, w_high, preferred_element_type=f32)
            + jnp.dot(x_high, w_low, preferred_element_type=f32)
        )
        tr = jnp.tanh(0.5 * pre[:, :SPAN])
        ti = jnp.tanh(0.5 * pre[:, SPAN:])
        recur = 0.5 + 0.5 * tr
        inp = 0.5 + 0.5 * ti
        rate = tiled(rows[4:5, :])
        log = rate * recur + fed_s[here, :]
        decay = jnp.exp(log)
        square = decay * decay
        u = 2.0 * log
        series = -u * (1 + u * (1 / 2) * (1 + u * (1 / 3) * (1 + u * (1 / 4) * (1 + u * (1 / 5) * (1 + u * (1 / 6))))))
        left_over = jnp.where(u > -0.25, series, 1.0 - square)
        inverse = lax.rsqrt(left_over)
        root = left_over * inverse
        fed = inp * x
        pushed = root * fed
        decay_s[here, :] = decay
        fed_s[here, :] = pushed
        slope_s[here, :] = square * inverse * fed
        rate_s[here, :] = rate * (0.25 - 0.25 * tr * tr)
        recur_s[here, :] = recur
        c0_o[here, :] = (root * inp).astype(bf16)
        c1_o[here, :] = (pushed * (0.5 - 0.5 * ti)).astype(bf16)
        turned_o[:, here] = jnp.transpose(x_high)
        return 0

    lax.fori_loop(0, 8, gates, 0, unroll=8)
    next_o[0:1016, :] = decay_s[8:1024, :]
    next_o[1016:1024, :] = after_of(decay_s[0:8, :])
    for copy in copies[1:6]:
        copy.start()
    local_s[0:8, :] = jnp.zeros((8, SPAN), f32)
    power_s[0:8, :] = jnp.ones((8, SPAN), f32)

    def scan(n, held):
        value, power = held
        for m in range(8):
            at = pl.ds(pl.multiple_of(n * 64 + 8 * m, 8), 8)
            a = decay_s[at, :]
            value = fed_s[at, :] + a * value
            power = a * power
            to = pl.ds(pl.multiple_of(n * 64 + 8 * m + 8, 8), 8)
            local_s[to, :] = value
            power_s[to, :] = power
        return value, power

    value, power = lax.fori_loop(0, 16, scan, (jnp.zeros((8, SPAN), f32), jnp.ones((8, SPAN), f32)))
    enters = jnp.broadcast_to(entering(power, value, False)[None], (16, 8, SPAN)).reshape(SPAN, SPAN)

    def slopes(n, _):
        here = block_of(n)
        previous = local_s[here, :] + power_s[here, :] * enters
        decay = decay_s[here, :]
        slope = previous * decay - slope_s[here, :]
        c2_o[here, :] = (slope * rate_s[here, :]).astype(bf16)
        c3_o[here, :] = (slope * recur_s[here, :]).astype(bf16)
        state_s[here, :] = local_s[moved_block(n, 8), :] + power_s[moved_block(n, 8), :] * enters
        return 0

    lax.fori_loop(0, 8, slopes, 0)
    for copy in copies[6:8]:
        copy.start()
    for p in range(8):
        state = jnp.transpose(strided(state_s, p))
        for half in range(2):
            at = slice((8 * half + p) * SPAN, (8 * half + p + 1) * SPAN)
            turn = gelu_parts(gate[:, at].astype(f32))[1]
            g1_o[:, at] = (state[GROUP * half : GROUP * half + GROUP] * turn).astype(bf16)
    copies[8].start()
    for copy in copies:
        copy.wait()


def backward_kernel(
    cot, next_r, c0_r, c1_r, c2_r, c3_r, branch_r, turned_r, g0_r, back_r, rows,
    gb_o, small_o, d_s, local_s, power_s, dx_s, pushed_s,
):
    for p in range(8):
        parts = []
        for j in (p, 8 + p):
            at = slice(j * SPAN, (j + 1) * SPAN)
            c = cot[j].astype(f32)
            parts.append(c * g0_r[:, at].astype(f32))
        d_s[pl.ds(p, SPAN, stride=8), :] = jnp.transpose(halves(*parts))

    def scan(n, held):
        value, power = held
        for m in range(8):
            at = pl.ds(pl.multiple_of(1016 - n * 64 - 8 * m, 8), 8)
            a = next_r[at, :]
            value = d_s[at, :] + a * value
            power = a * power
            local_s[at, :] = value
            power_s[at, :] = power
        return value, power

    value, power = lax.fori_loop(0, 16, scan, (jnp.zeros((8, SPAN), f32), jnp.ones((8, SPAN), f32)))
    enters = jnp.broadcast_to(entering(power, value, True)[None], (16, 8, SPAN)).reshape(SPAN, SPAN)

    def summed(block):
        return jnp.sum(block.reshape(16, 8, SPAN), axis=0)

    def spread(n, total):
        here = block_of(n)
        grad = local_s[here, :] + power_s[here, :] * enters
        high = jnp.concatenate(
            [(grad * c2_r[here, :].astype(f32)).astype(bf16), (grad * c1_r[here, :].astype(f32)).astype(bf16)], axis=1
        )
        pushed_s[here, :] = high
        back = jnp.dot(high, back_r[0], preferred_element_type=f32) + jnp.dot(
            high, back_r[1], preferred_element_type=f32
        )
        dx_s[here, :] = grad * c0_r[here, :].astype(f32) + back
        return total + summed(grad * c3_r[here, :].astype(f32))

    zero = jnp.zeros((8, SPAN), f32)
    decays = lax.fori_loop(0, 8, spread, zero, unroll=8)
    for m in range(3):
        dx_s[1024 + 8 * m : 1032 + 8 * m, :] = after_of(dx_s[8 * m : 8 * m + 8, :])

    def taps(n, totals):
        here = block_of(n)
        value = branch_r[here, :].astype(f32)
        gb, out = None, []
        for k in range(CONV):
            dx = dx_s[moved_block(n, 8 * (3 - k)), :]
            term = tiled(rows[k : k + 1, :]) * dx
            gb = term if gb is None else gb + term
            out.append(totals[k] + summed(value * dx))
        d_s[here, :] = gb
        return tuple(out)

    totals = lax.fori_loop(0, 8, taps, (zero,) * CONV, unroll=8)
    for p in range(8):
        gb = jnp.transpose(strided(d_s, p)).astype(bf16)
        gb_o[p] = gb[:GROUP]
        gb_o[8 + p] = gb[GROUP:]
    product = jnp.dot(turned_r[...], pushed_s[...], preferred_element_type=f32)
    low = lanes((GROUP, SPAN)) < GROUP
    r_part = product[:GROUP, :SPAN] + pltpu.roll(product[GROUP:, :SPAN], GROUP, 1)
    i_part = pltpu.roll(product[:GROUP, SPAN:], GROUP, 1) + product[GROUP:, SPAN:]
    small_o[0:GROUP, :] = jnp.where(low, r_part, i_part).astype(bf16)
    row = lax.broadcasted_iota(jnp.int32, (8, SPAN), 0)
    table = zero
    for k, total in enumerate((*totals, decays * jnp.broadcast_to(rows[5:6, :], (8, SPAN)))):
        flat = jnp.broadcast_to(jnp.sum(total, axis=0, keepdims=True), (8, SPAN))
        table = jnp.where(row == k, flat + pltpu.roll(flat, GROUP, 1), table)
    small_o[GROUP : GROUP + 8, :] = table.astype(bf16)


VMEM = pl.BlockSpec(memory_space=pltpu.VMEM)
ANY = pl.BlockSpec(memory_space=pl.ANY)
FLAT = (1024, SPAN)


def here_in_vmem(array):
    return pltpu.with_memory_space_constraint(array, pltpu.VMEM)


def forward_part(branch, gate, shift, conv, decay_param, recur_map, input_map):
    flat = [(FLAT, f32)] + [(FLAT, bf16)] * 5 + [((SPAN, 1024), bf16)] + [(branch.shape, bf16)] * 2
    ends = [((2, 2 * SPAN, SPAN), bf16), ((8, SPAN), f32)]
    return pl.pallas_call(
        forward_kernel,
        in_specs=[VMEM] * 7,
        out_specs=[ANY] * 9 + [VMEM] * 2,
        out_shape=[jax.ShapeDtypeStruct(*each) for each in (*flat, *ends)],
        scratch_shapes=[pltpu.VMEM(*each) for each in flat]
        + [pltpu.VMEM((1048, SPAN), f32)]
        + [pltpu.VMEM(FLAT, f32)] * 5
        + [pltpu.VMEM((1032, SPAN), f32)] * 2
        + [pltpu.VMEM(FLAT, f32), pltpu.SemaphoreType.DMA((9,))],
        name="forward_part",
    )(branch, gate, shift, conv, decay_param, recur_map, input_map)


def backward_part(cot, saved):
    return pl.pallas_call(
        backward_kernel,
        out_shape=[
            jax.ShapeDtypeStruct((16, GROUP, SPAN), bf16),
            jax.ShapeDtypeStruct((GROUP + 8, 2 * GROUP), bf16),
        ],
        scratch_shapes=[pltpu.VMEM(FLAT, f32)] * 3 + [pltpu.VMEM((1048, SPAN), f32), pltpu.VMEM((1024, 2 * SPAN), bf16)],
        name="backward_part",
    )(cot, *saved)


def product_kernel(place, small, partner, own, near, far, grads, out):
    total = None
    blocks = (own[...], near[0:1024, :], far[0, 0:1024, :], far[1, 0:1024, :])
    for n, block in enumerate(blocks):
        theirs = grads[:, place[0] ^ NEAREST[n]].reshape(256, SPAN)
        term = lax.dot_general(block, theirs, (((1,), (1,)), ((), ())), preferred_element_type=f32)
        total = term if total is None else total + term
    pieces = out.shape[0]
    out[:, 0:32, :] = total.astype(bf16).reshape(pieces, 32, 256)
    mine = pl.ds(pl.multiple_of(place[2] * 32, 32), 32)
    maps = (small[mine, :].astype(f32) + partner[mine, :].astype(f32)).astype(bf16)
    rest = (small[64:72, :].astype(f32) + partner[64:72, :].astype(f32)).astype(bf16)
    top = jnp.concatenate([maps[0:16], maps[16:32]], axis=1)
    low = jnp.concatenate([rest, jnp.zeros((8, SPAN), bf16)], axis=1)
    out[:, 32:56, :] = jnp.broadcast_to(jnp.concatenate([top, low], axis=0)[None], (pieces, 24, 256))


def gather_sum_kernel(arrived, packed_o, conv_o, recur_o, input_o, decay_o):
    block = lax.broadcasted_iota(jnp.int32, (16, SPAN), 1) // 16
    totals = []
    for n in range(4):
        total = arrived[8 * n, 0:32, :].astype(f32)
        for m in range(1, 8):
            total = total + arrived[8 * n + m, 0:32, :].astype(f32)
        totals.append(total)
    for core in range(2):
        extra = arrived[core, 32:56, :].astype(f32)
        for n in range(core + 2, 32, 2):
            extra = extra + arrived[n, 32:56, :].astype(f32)
        for n in range(2):
            at = slice(32 * core + 16 * n, 32 * core + 16 * n + 16)
            half = extra[0:16, n * SPAN : (n + 1) * SPAN]
            recur_o[at, :] = half[:, 0:GROUP]
            input_o[at, :] = pltpu.roll(half, GROUP, 1)[:, 0:GROUP]
        if core == 0:
            conv_o[...] = extra[16:20, 0:GROUP]
            decay_o[...] = extra[20:21, 0:GROUP]
    for group in range(16):
        tile = slice((group // 8) * SPAN, (group // 8 + 1) * SPAN)
        piece = None
        for j in range(8):
            source = totals[j % 4][16 * (j // 4) : 16 * (j // 4) + 16, tile]
            shift = (16 * (j - group % 8)) % SPAN
            turned = pltpu.roll(source, shift, 1) if shift else source
            piece = turned if piece is None else jnp.where(block == j, turned, piece)
        packed_o[group] = piece.astype(bf16)


def last_sum_kernel(arrived, out):
    total = arrived[0].astype(f32)
    for n in range(1, arrived.shape[0]):
        total = total + arrived[n].astype(f32)
    out[0:16, :] = total[:, 0:GROUP]
    out[16:32, :] = pltpu.roll(total, GROUP, 1)[:, 0:GROUP]


def token_grad_kernel(place, close, away, close_other, away_other, own, one, two, three, cot, g1, out, gate_o, tokens_s):
    for j in range(cot.shape[0]):
        at = slice(j * SPAN, (j + 1) * SPAN)
        gate_o[:, at] = (cot[j].astype(f32) * g1[:, at].astype(f32)).astype(bf16)
    for n, piece in enumerate((own, one, two, three)):
        tokens_s[:, place[0] ^ n] = piece[...]
    tokens = tokens_s[...].reshape(1024, SPAN)
    for part, half in enumerate((close, away, close_other, away_other)):
        tiles = half[...].reshape(8, 4, 8, 8, SPAN)
        result = None
        for n in range(8):
            term = jnp.dot(
                tiles[:, :, n].reshape(256, SPAN), tokens[n * SPAN : (n + 1) * SPAN], preferred_element_type=f32
            )
            result = term if result is None else result + term
        result = result.astype(bf16)
        for n in range(8):
            y, x = place[0] ^ NEAREST[n % 4], place[1] ^ NEAREST[n // 4 + 2 * (part % 2)]
            row = ((y * 4 + x) * 2 + (place[2] ^ (part // 2))) * 32
            out[pl.ds(pl.multiple_of(row, 32), 32), :] = result[32 * n : 32 * n + 32]


def exchanged(array, axis, bit):
    size = lax.axis_size(axis)
    return lax.ppermute(array, axis, [(n, n ^ bit) for n in range(size)])


def joined(array, axis, bits):
    both = lax.optimization_barrier((array, exchanged(array, axis, bits)))
    return jnp.concatenate(both, axis=0)


def steps(
    normed, branch_in, gate_pre, cotangent, decay_shift,
    conv_weight, recur_weight, input_weight, decay_param, branch_proj,
):
    spans = lax.axis_size("sp")
    cot = lax.all_to_all(cotangent[0].reshape(spans, GROUP, SPAN), "sp", 0, 0, tiled=True)
    *saved, g1, back_maps, taps = forward_part(
        here_in_vmem(branch_in[0]), here_in_vmem(gate_pre[0]), decay_shift.reshape(spans, SPAN),
        conv_weight, decay_param[None], recur_weight[0], input_weight[0],
    )
    saved = [*map(here_in_vmem, saved[:4]), *saved[4:], back_maps, taps]
    own = normed[0]
    width = branch_proj.shape[1] // SPAN
    rows = branch_proj.reshape(4, 8, width, SPAN).transpose(0, 2, 1, 3).reshape(-1, SPAN)
    packed = jnp.concatenate([own, rows], axis=0)
    near = exchanged(packed, "y", 1)
    far = exchanged(jnp.stack([packed, near]), "y", 3)
    held = jnp.stack([rows, near[1024:], far[0, 1024:], far[1, 1024:]])
    close = joined(held, "x", 1)
    away = exchanged(close, "x", 3)
    halves_here = (close, away, exchanged(close, "core", 1), exchanged(away, "core", 1))
    gb, small = backward_part(here_in_vmem(cot), saved)
    partner = exchanged(small, "core", 1)
    grads = lax.all_to_all(gb.reshape(64, 16, SPAN), ("sp", "y"), 0, 0, tiled=True)
    grads = grads.reshape(16, 4, 16, SPAN)
    here = lax.axis_index("y")
    place = jnp.stack([lax.axis_index(axis) for axis in DP]).astype(jnp.int32)
    smem = pl.BlockSpec(memory_space=pltpu.SMEM)
    pieces = pl.pallas_call(
        product_kernel,
        in_specs=[smem] + [VMEM] * 6,
        out_specs=VMEM,
        out_shape=jax.ShapeDtypeStruct((32, 56, 256), bf16),
        name="product",
    )(place, small, here_in_vmem(partner), own, here_in_vmem(near), here_in_vmem(far), here_in_vmem(grads))
    arrived = lax.all_to_all(pieces, DP, 0, 0, tiled=True)

    def part_for(n):
        return lax.dynamic_index_in_dim(grads, here ^ n, 1, keepdims=False)

    own_part = part_for(0)
    others = [exchanged(part_for(n), "y", n) for n in (1, 2, 3)]
    sums, grad_conv, grad_recur, grad_input, grad_decay = pl.pallas_call(
        gather_sum_kernel,
        out_shape=[
            jax.ShapeDtypeStruct((16, 16, SPAN), bf16),
            jax.ShapeDtypeStruct((CONV, GROUP), f32),
            jax.ShapeDtypeStruct((GROUP, GROUP), f32),
            jax.ShapeDtypeStruct((GROUP, GROUP), f32),
            jax.ShapeDtypeStruct((1, GROUP), f32),
        ],
        name="gather_sum",
    )(here_in_vmem(arrived))
    last = lax.all_to_all(sums, "sp", 0, 0, tiled=True)
    grad_proj = pl.pallas_call(
        last_sum_kernel, out_shape=jax.ShapeDtypeStruct((32, GROUP), f32), name="last_sum"
    )(here_in_vmem(last))
    grad_normed, grad_gate = pl.pallas_call(
        token_grad_kernel,
        in_specs=[smem] + [VMEM] * 10,
        out_specs=[VMEM] * 2,
        out_shape=[jax.ShapeDtypeStruct((1024, SPAN), bf16), jax.ShapeDtypeStruct(g1.shape, bf16)],
        scratch_shapes=[pltpu.VMEM((16, 4, 16, SPAN), bf16)],
        name="token_grad",
    )(place, *halves_here[:2], *map(here_in_vmem, halves_here[2:]), *map(here_in_vmem, (own_part, *others)), cot, g1)
    return (
        grad_normed[None],
        grad_gate[None],
        grad_proj,
        grad_conv,
        grad_recur[None],
        grad_input[None],
        grad_decay[0],
    )


def solution(mesh):
    split = Mesh(mesh.devices.reshape(16, 4, 4, 2), ("sp", *DP))
    return jax.shard_map(
        steps,
        mesh=split,
        in_specs=(
            P(DP, None, "sp"),
            P(DP, "sp", None),
            P(DP, "sp", None),
            P(DP, None, "sp"),
            P(DP, "sp", None),
            P(None, "sp"),
            P("sp", None, None),
            P("sp", None, None),
            P("sp"),
            P(DP, None),
        ),
        out_specs=(
            P(DP, None, "sp"),
            P(DP, "sp", None),
            P(DP, "sp"),
            P(None, "sp"),
            P("sp", None, None),
            P("sp", None, None),
            P("sp"),
        ),
        check_vma=False,
    )
```
